32 devices in a mesh: sp: 4 (over z), fs: 4 (over y, core), tp: 2 (over x).
Axes of the slice: x: 2, y: 2, z: 4, core: 2. Of those that a mesh axis runs over, the one named last changes fastest.
Arguments:
- input_layer_rows: bfloat16 [4, 1024, 2048], P('fs', 'sp'), may hold values from -6 to 6
- input_norm_gain: float32 [2048], replicated, may hold values from 0.1 to 1.9
- query_weight_attention: bfloat16 [2048, 1024], P(('sp', 'fs'), 'tp'), may hold values from -0.125 to 0.125
- key_weight_attention: bfloat16 [2048, 1024], P(('sp', 'fs'), 'tp'), may hold values from -0.125 to 0.125
- value_weight_attention: bfloat16 [2048, 1024], P(('sp', 'fs'), 'tp'), may hold values from -0.125 to 0.125
- query_weight_recurrent: bfloat16 [2048, 1024], P(('sp', 'fs'), 'tp'), may hold values from -0.125 to 0.125
- forget_weight_recurrent: bfloat16 [2048, 1024], P(('sp', 'fs'), 'tp'), may hold values from -0.125 to 0.125
- value_weight_recurrent: bfloat16 [2048, 1024], P(('sp', 'fs'), 'tp'), may hold values from -0.125 to 0.125
- gate_weight_recurrent: bfloat16 [2048, 1024], P(('sp', 'fs'), 'tp'), may hold values from -0.125 to 0.125
- output_weight_attention: bfloat16 [2048, 1024], P(('sp', 'fs'), 'tp'), may hold values from -0.125 to 0.125
- emitted_projection_linear_scan: bfloat16 [2048, 1024], P(('sp', 'fs'), 'tp'), may hold values from -0.125 to 0.125
- score_offset: float32 [8], P('tp'), as said below
- attention_norm_gain: float32 [1024], P('tp'), may hold values from 0.1 to 1.9
- recurrence_norm_gain: float32 [1024], P('tp'), may hold values from 0.1 to 1.9
- forget_floor: float32 [1024], P('tp'), may hold values from 0.1 to 0.5
- forget_offset: float32 [1024], P('tp'), as said below
- extra_log_decay: float32 [4, 1024, 1024], P('fs', 'sp', 'tp')
Outputs:
- layer_out: bfloat16 [4, 1024, 2048], P('fs', ('sp', 'tp'))
- row_log_total: float32 [4, 8, 1024], P('fs', 'tp', 'sp')
The draws below stay inside these ranges and needn't reach their ends.
Inputs may be any that keep to these rules, and one draw needn't show every extreme that they name: `score_offset`: each head's offset lies between -ln(1024) - 2 and -ln(1024) + 0.5. `forget_offset`: each channel's offset lies between ln(256) - 3 and ln(1024) + 0.6.
All inputs are finite; a program needn't handle non-finite values.
Results may differ from the reference program's by a relative error of at most 0.015.
Values may be sent and summed in bfloat16 or wider, within the bound.
A program may use at most 64 MiB of HBM per device.

```python
import math
import jax
import jax.numpy as jnp
from jax import lax

HEAD = 128
HEADS = 8
D_HALF = 1024
D = 2048
TOK_DEV = 256
BLOCK = 64
SEQ = 1024
BATCH = 4


def draw_score_offset(key, part):
    center = -math.log(SEQ)
    return jax.random.uniform(key, (HEADS,), jnp.float32, center - 2.0, center + 0.5)


def draw_forget_offset(key, part):
    width = HEADS * HEAD
    first, second, third = jax.random.split(key, 3)
    chooser = jax.random.uniform(first, (width,), jnp.float32)
    slow_value = math.log(SEQ) + jax.random.uniform(second, (width,), jnp.float32, -0.4, 0.6)
    fast_value = math.log(TOK_DEV) - 2.5 + jax.random.uniform(third, (width,), jnp.float32, -0.5, 0.5)
    share = 0.5
    return jnp.where(chooser < share, fast_value, slow_value)


def draw_extra_log_decay(key, part):
    width = HEADS * HEAD
    first, second, third = jax.random.split(key, 3)
    blocks = SEQ // TOK_DEV
    lowest, highest_score = (0.05, 0.4)
    rates = jnp.exp(jax.random.uniform(first, (BATCH, blocks, 1, width), jnp.float32, math.log(lowest), math.log(highest_score))) / SEQ
    constant_component = jnp.broadcast_to(rates, (BATCH, blocks, TOK_DEV, width)).reshape(BATCH, SEQ, width)
    spots = jax.random.randint(second, (BATCH, 3), 0, SEQ)
    stratum_level = jnp.log(jax.random.uniform(third, (BATCH, 3, width), jnp.float32, 0.6, 0.85))
    equality_indicators = (jnp.arange(SEQ)[None, :, None] == spots[:, None, :]).astype(jnp.float32)
    fading_spikes = jnp.einsum('tsk,tkx->tsx', equality_indicators, stratum_level, precision=jax.lax.Precision.HIGHEST)
    return fading_spikes - constant_component


def level_of(rng, extent, shards, smallest, high):
    level, own = 1.0, jax.random.fold_in(rng, 6)
    for axis_at, shards_of in shards:
        heights = jnp.exp(jax.random.uniform(jax.random.fold_in(own, axis_at), (shards_of,), jnp.float32, smallest / len(shards), high / len(shards)))
        level = level * jnp.repeat(heights, extent[axis_at] // shards_of).reshape([-1 if axis == axis_at else 1 for axis in range(len(extent))])
    return level


def normal_values(key, dims, spread, reach, pieces=(), held_as=jnp.bfloat16):
    level = level_of(key, dims, pieces, -0.22, 0.18) if pieces else 1.0
    result = jax.random.normal(key, dims, jnp.float32) * spread * level
    return jnp.minimum(jnp.maximum(result, -reach), reach).astype(held_as)


def setup_inputs(seed: int = 0) -> dict:
    key_of = jax.random.split(jax.random.key(seed), 18)
    input_layer_rows = normal_values(key_of[0], (BATCH, SEQ, D), 1.0, 6.0, ((0, 4), (1, 4)))
    input_norm_gain = jnp.clip(1.0 + 0.18 * jax.random.normal(key_of[1], (D,), jnp.float32), 0.1, 1.9)
    query_weight_attention = normal_values(key_of[2], (D, D_HALF), D ** -0.5, 0.125, ((0, 16), (1, 2)))
    key_weight_attention = normal_values(key_of[3], (D, D_HALF), D ** -0.5, 0.125, ((0, 16), (1, 2)))
    value_weight_attention = normal_values(key_of[4], (D, D_HALF), D ** -0.5, 0.125, ((0, 16), (1, 2)))
    query_weight_recurrent = normal_values(key_of[5], (D, D_HALF), D ** -0.5, 0.125, ((0, 16), (1, 2)))
    forget_weight_recurrent = normal_values(key_of[6], (D, D_HALF), D ** -0.5, 0.125, ((0, 16), (1, 2)))
    value_weight_recurrent = normal_values(key_of[7], (D, D_HALF), D ** -0.5, 0.125, ((0, 16), (1, 2)))
    gate_weight_recurrent = normal_values(key_of[8], (D, D_HALF), D ** -0.5, 0.125, ((0, 16), (1, 2)))
    output_weight_attention = normal_values(key_of[9], (D, D_HALF), D ** -0.5, 0.125, ((0, 16), (1, 2)))
    emitted_projection_linear_scan = normal_values(key_of[10], (D, D_HALF), D ** -0.5, 0.125, ((0, 16), (1, 2)))
    score_offset = draw_score_offset(jax.random.fold_in(key_of[17], 71), 0)
    attention_norm_gain = jnp.clip(1.0 + 0.18 * jax.random.normal(key_of[12], (D_HALF,), jnp.float32), 0.1, 1.9)
    recurrence_norm_gain = jnp.clip(1.0 + 0.18 * jax.random.normal(key_of[13], (D_HALF,), jnp.float32), 0.1, 1.9)
    forget_floor = jnp.clip(0.1 + 0.4 * jax.random.uniform(key_of[14], (D_HALF,), jnp.float32) ** level_of(key_of[14], (D_HALF,), ((0, 2),), -0.2, 0.2), 0.1, 0.5)
    forget_offset = draw_forget_offset(jax.random.fold_in(key_of[17], 71), 0)
    extra_log_decay = draw_extra_log_decay(jax.random.fold_in(key_of[17], 71), 0)
    return {"input_layer_rows": input_layer_rows, "input_norm_gain": input_norm_gain, "query_weight_attention": query_weight_attention, "key_weight_attention": key_weight_attention, "value_weight_attention": value_weight_attention, "query_weight_recurrent": query_weight_recurrent, "forget_weight_recurrent": forget_weight_recurrent, "value_weight_recurrent": value_weight_recurrent, "gate_weight_recurrent": gate_weight_recurrent, "output_weight_attention": output_weight_attention, "emitted_projection_linear_scan": emitted_projection_linear_scan, "score_offset": score_offset, "attention_norm_gain": attention_norm_gain, "recurrence_norm_gain": recurrence_norm_gain, "forget_floor": forget_floor, "forget_offset": forget_offset, "extra_log_decay": extra_log_decay}


epsilon = 1e-06
log_floor = 0.05

def normalize_rows(inputs, gain):
    values = inputs.astype(jnp.float32)
    square_mean = lax.optimization_barrier(jnp.mean(values * values, axis=-1, keepdims=True))
    return values * lax.rsqrt(square_mean + epsilon) * gain

def head_norm(values, gain):
    square_mean = lax.optimization_barrier(jnp.mean(values * values, axis=-1, keepdims=True))
    return values * lax.rsqrt(square_mean + epsilon) * gain

def project(normed, weight):
    return jnp.dot(normed, weight, preferred_element_type=jnp.float32).astype(jnp.bfloat16)

def recurrence_block(memory_matrix, inputs):
    query_slice, decay_part, key_slice, value_slice = inputs
    highest_score = lax.Precision.HIGHEST
    length = decay_part.shape[0]
    running_total = jnp.cumsum(decay_part, axis=0)
    causal = (lax.broadcasted_iota(jnp.int32, (length, length), 0) >= lax.broadcasted_iota(jnp.int32, (length, length), 1))[:, :, None, None]
    relative = jnp.where(causal, running_total[:, None] - running_total[None, :], -jnp.inf)
    pairwise = lax.optimization_barrier(jnp.sum(query_slice[:, None] * key_slice[None, :] * jnp.exp(relative), axis=-1))
    inner_part = jnp.einsum('tsh,shv->thv', pairwise, value_slice, precision=highest_score)
    carried_state = jnp.einsum('fby,bym->fbm', query_slice * jnp.exp(running_total), memory_matrix, precision=highest_score)
    final_total = running_total[-1]
    updated_state = jnp.exp(final_total)[:, :, None] * memory_matrix + jnp.einsum('rxc,rxa->xca', key_slice * jnp.exp(final_total[None] - running_total), value_slice, precision=highest_score)
    return (updated_state, inner_part + carried_state)

def recurrence(query_rows_input, forget_log_value, key_in, value_in):
    seq_len = query_rows_input.shape[0]

    def to_blocks(array_in):
        return array_in.reshape(seq_len // BLOCK, BLOCK, HEADS, HEAD)
    initial = jnp.zeros((HEADS, HEAD, HEAD), jnp.float32)
    unused, outputs = lax.scan(recurrence_block, initial, (to_blocks(query_rows_input), to_blocks(forget_log_value), to_blocks(key_in), to_blocks(value_in)))
    return outputs.reshape(seq_len, HEADS, HEAD)

def stick_attention(queries, keys_all, values_all, shifts):
    outputs = []
    totals = []
    for block_index in range(SEQ // TOK_DEV):
        first = block_index * TOK_DEV
        final = first + TOK_DEV
        scores = jnp.einsum('thd,shd->hts', queries[first:final].astype(jnp.float32), keys_all[:final].astype(jnp.float32)) * HEAD ** (-0.5) + shifts[:, None, None]
        strict = first + lax.broadcasted_iota(jnp.int32, (TOK_DEV, final), 0) > lax.broadcasted_iota(jnp.int32, (TOK_DEV, final), 1)
        logarithmic_retention = jnp.where(strict, jax.nn.log_sigmoid(-scores), 0.0)
        suffix = lax.cumsum(logarithmic_retention, axis=2, reverse=True) - logarithmic_retention
        log_weight = jnp.where(strict, jax.nn.log_sigmoid(scores) + suffix, -jnp.inf)
        weights = jnp.exp(log_weight).astype(jnp.bfloat16)
        outputs.append(jnp.einsum('hts,shd->thd', weights.astype(jnp.float32), values_all[:final].astype(jnp.float32)))
        totals.append(lax.optimization_barrier(jnp.sum(logarithmic_retention, axis=2)))
    return (jnp.concatenate(outputs, axis=0), jnp.concatenate(totals, axis=1))

def reference(input_layer_rows, input_norm_gain, query_weight_attention, key_weight_attention, value_weight_attention, query_weight_recurrent, forget_weight_recurrent, value_weight_recurrent, gate_weight_recurrent, output_weight_attention, emitted_projection_linear_scan, score_offset, attention_norm_gain, recurrence_norm_gain, forget_floor, forget_offset, extra_log_decay):
    layer_rows = []
    log_rows = []
    for batch_position in range(BATCH):
        normed = normalize_rows(input_layer_rows[batch_position], input_norm_gain).astype(jnp.bfloat16)
        query_a = project(normed, query_weight_attention).reshape(SEQ, HEADS, HEAD)
        key_a = project(normed, key_weight_attention).reshape(SEQ, HEADS, HEAD)
        value_a = project(normed, value_weight_attention).reshape(SEQ, HEADS, HEAD)
        query_b = project(normed, query_weight_recurrent)
        forget_b = project(normed, forget_weight_recurrent)
        input_b = project(normed, value_weight_recurrent)
        gate_b = project(normed, gate_weight_recurrent)
        attended, keep_total = stick_attention(query_a, key_a, value_a, score_offset)
        log_rows.append(jnp.log(jnp.maximum(-jnp.expm1(keep_total), log_floor)))
        mixed_a = head_norm(attended, attention_norm_gain.reshape(HEADS, HEAD)).reshape(SEQ, D_HALF).astype(jnp.bfloat16)
        forget_logits = forget_b.astype(jnp.float32) + forget_offset
        forget_log_value = jnp.logaddexp(jnp.log(forget_floor), jnp.log1p(-forget_floor) + jax.nn.log_sigmoid(forget_logits)) + extra_log_decay[batch_position]
        key_in = (1.0 - forget_floor) * jax.nn.sigmoid(-forget_logits)
        query_rows_input = jax.nn.silu(query_b.astype(jnp.float32))
        value_in = input_b.astype(jnp.float32)
        recurrent = recurrence(query_rows_input.reshape(SEQ, HEADS, HEAD), forget_log_value.reshape(SEQ, HEADS, HEAD), key_in.reshape(SEQ, HEADS, HEAD), value_in.reshape(SEQ, HEADS, HEAD))
        gated_out = head_norm(recurrent, recurrence_norm_gain.reshape(HEADS, HEAD)) * jax.nn.silu(gate_b.astype(jnp.float32).reshape(SEQ, HEADS, HEAD))
        mixed_b = gated_out.reshape(SEQ, D_HALF).astype(jnp.bfloat16)
        summed = jnp.dot(mixed_a, output_weight_attention.T, preferred_element_type=jnp.float32) + jnp.dot(mixed_b, emitted_projection_linear_scan.T, preferred_element_type=jnp.float32)
        layer_rows.append(summed.astype(jnp.bfloat16))
    return (jnp.stack(layer_rows), jnp.stack(log_rows))
```

```python
import functools
import jax
import jax.numpy as jnp
from jax import lax
from jax.experimental import pallas as pl
from jax.experimental.pallas import tpu as pltpu
from jax.sharding import PartitionSpec as P

HEAD = 128
BLOCK = 64


epsilon = 1e-06
log_floor = 0.05


def entering(shard, axis, combine, identity):
    size, index = (lax.axis_size(axis), lax.axis_index(axis))
    everything = jax.tree.map(
        lambda part, kind: lax.all_gather(part.astype(kind), axis),
        shard,
        (jnp.bfloat16, jnp.bfloat16),
    )
    start = jax.tree.map(
        lambda part, zero: jnp.broadcast_to(jnp.asarray(zero, part.dtype), part.shape),
        shard,
        identity,
    )

    def hop(k, before):
        reached = k < index
        new = combine(
            before, jax.tree.map(lambda part, own: part[k].astype(own.dtype), everything, shard)
        )
        return jax.tree.map(lambda a, b: jnp.where(reached, a, b), new, before)

    return lax.fori_loop(0, size, hop, start)


def head_norm(values, gain):
    square_mean = jnp.mean(values * values, axis=-1, keepdims=True)
    return values * lax.rsqrt(square_mean + epsilon) * gain


def recurrence_block(memory_matrix, inputs):
    query_slice, decay_part, key_slice, value_slice = inputs
    highest_score = lax.Precision.HIGHEST
    length = decay_part.shape[0]
    running_total = jnp.cumsum(decay_part, axis=0)
    causal = (
        lax.broadcasted_iota(jnp.int32, (length, length), 0)
        >= lax.broadcasted_iota(jnp.int32, (length, length), 1)
    )[:, :, None, None]
    relative = jnp.where(causal, running_total[:, None] - running_total[None, :], -jnp.inf)
    pairwise = jnp.sum(query_slice[:, None] * key_slice[None, :] * jnp.exp(relative), axis=-1)
    inner_part = jnp.einsum("tsh,shv->thv", pairwise, value_slice, precision=highest_score)
    carried_state = jnp.einsum(
        "fby,bym->fbm", query_slice * jnp.exp(running_total), memory_matrix, precision=highest_score
    )
    final_total = running_total[-1]
    updated_state = jnp.exp(final_total)[:, :, None] * memory_matrix + jnp.einsum(
        "rxc,rxa->xca",
        key_slice * jnp.exp(final_total[None] - running_total),
        value_slice,
        precision=highest_score,
    )
    return (updated_state, inner_part + carried_state)


def stick_piece(queries, shifts, weighted, keep_total, key_value, is_own, is_valid):
    scores = (
        jnp.einsum("thd,shd->hts", queries, key_value[0], preferred_element_type=jnp.float32)
        * HEAD ** (-0.5)
        + shifts[:, None, None]
    )
    logarithmic_retention = jax.nn.log_sigmoid(-scores)
    if is_own:
        rows_here = scores.shape[1]
        strict = lax.broadcasted_iota(jnp.int32, (rows_here, rows_here), 0) > lax.broadcasted_iota(
            jnp.int32, (rows_here, rows_here), 1
        )
        logarithmic_retention = jnp.where(strict, logarithmic_retention, 0.0)
    suffix = lax.cumsum(logarithmic_retention, axis=2, reverse=True) - logarithmic_retention
    log_weight = jax.nn.log_sigmoid(scores) + suffix + keep_total[:, :, None]
    if is_own:
        log_weight = jnp.where(strict, log_weight, -jnp.inf)
    weights = jnp.where(is_valid, jnp.exp(log_weight), 0.0).astype(jnp.bfloat16)
    weighted = weighted + jnp.einsum(
        "hts,shd->thd", weights, key_value[1], preferred_element_type=jnp.float32
    )
    keep_total = keep_total + jnp.where(is_valid, jnp.sum(logarithmic_retention, axis=2), 0.0)
    return (weighted, keep_total)


def contract_rows(rows_in, weight):
    return lax.dot_general(
        rows_in, weight, (((1,), (1,)), ((), ())), preferred_element_type=jnp.float32
    )


def on_device_general(
    input_layer_rows,
    input_norm_gain,
    query_weight_attention,
    key_weight_attention,
    value_weight_attention,
    query_weight_recurrent,
    forget_weight_recurrent,
    value_weight_recurrent,
    gate_weight_recurrent,
    output_weight_attention,
    emitted_projection_linear_scan,
    score_offset,
    attention_norm_gain,
    recurrence_norm_gain,
    forget_floor,
    forget_offset,
    extra_log_decay,
):
    values = input_layer_rows[0].astype(jnp.float32)
    square_mean = jnp.mean(values * values, axis=-1, keepdims=True)
    normed = (values * lax.rsqrt(square_mean + epsilon) * input_norm_gain).astype(jnp.bfloat16)
    tokens = normed.shape[0]
    weights_in = (
        query_weight_attention,
        key_weight_attention,
        value_weight_attention,
        query_weight_recurrent,
        forget_weight_recurrent,
        value_weight_recurrent,
        gate_weight_recurrent,
    )
    pieces = (
        lax.all_gather(weights_in[0], ("sp", "fs"), axis=0, tiled=True),
        lax.all_gather(weights_in[1], ("sp", "fs"), axis=0, tiled=True),
        lax.all_gather(weights_in[2], ("sp", "fs"), axis=0, tiled=True),
        lax.all_gather(weights_in[3], ("sp", "fs"), axis=0, tiled=True),
        lax.all_gather(weights_in[4], ("sp", "fs"), axis=0, tiled=True),
        lax.all_gather(weights_in[5], ("sp", "fs"), axis=0, tiled=True),
        lax.all_gather(weights_in[6], ("sp", "fs"), axis=0, tiled=True),
    )
    projected = tuple(
        (jnp.dot(normed, weight, preferred_element_type=jnp.float32) for weight in pieces)
    )
    query_a, key_a, value_a, query_b, forget_b, input_b, gate_b = [
        column_block.astype(jnp.bfloat16) for column_block in projected
    ]
    out_a, out_b = (
        lax.all_gather(output_weight_attention, ("sp", "fs"), axis=0, tiled=True),
        lax.all_gather(emitted_projection_linear_scan, ("sp", "fs"), axis=0, tiled=True),
    )
    head_count = query_a.shape[1] // HEAD
    queries = query_a.reshape(tokens, head_count, HEAD)
    key_value = jnp.stack(
        [key_a.reshape(tokens, head_count, HEAD), value_a.reshape(tokens, head_count, HEAD)]
    )
    weighted = jnp.zeros((tokens, head_count, HEAD), jnp.float32)
    keep_total = jnp.zeros((head_count, tokens), jnp.float32)
    weighted, keep_total = stick_piece(
        queries, score_offset, weighted, keep_total, key_value, True, True
    )
    position = lax.axis_index("sp")
    seq_devices = lax.axis_size("sp")
    gathered = lax.all_gather(key_value, "sp", axis=1, tiled=True)

    def gathered_turn(turn_index, carried_state):
        weighted_now, keep_now = carried_state
        source = jnp.maximum(position - turn_index, 0) * tokens
        piece_pair = lax.dynamic_slice_in_dim(gathered, source, tokens, 1)
        return stick_piece(
            queries, score_offset, weighted_now, keep_now, piece_pair, False, position >= turn_index
        )

    weighted, keep_total = lax.fori_loop(1, seq_devices, gathered_turn, (weighted, keep_total))
    row_log_total = jnp.log(jnp.maximum(-jnp.expm1(keep_total), log_floor))[None]
    mixed_a = (
        head_norm(weighted, attention_norm_gain.reshape(head_count, HEAD))
        .reshape(tokens, head_count * HEAD)
        .astype(jnp.bfloat16)
    )
    forget_logits = forget_b.astype(jnp.float32) + forget_offset
    forget_log_value = (
        jnp.logaddexp(
            jnp.log(forget_floor), jnp.log1p(-forget_floor) + jax.nn.log_sigmoid(forget_logits)
        )
        + extra_log_decay[0]
    )
    key_in = (1.0 - forget_floor) * jax.nn.sigmoid(-forget_logits)
    query_rows_input = jax.nn.silu(query_b.astype(jnp.float32)).reshape(tokens, head_count, HEAD)
    value_in = input_b.astype(jnp.float32)
    fading_channel_groups = forget_log_value.reshape(tokens, head_count, HEAD)
    shaped = tuple(
        (
            array_in.reshape(tokens // BLOCK, BLOCK, head_count, HEAD)
            for array_in in (query_rows_input, forget_log_value, key_in, value_in)
        )
    )
    empty_state = jnp.zeros((head_count, HEAD, HEAD), jnp.float32)
    nearby_hidden_vector, local_out = lax.scan(recurrence_block, empty_state, shaped)
    local_out = local_out.reshape(tokens, head_count, HEAD)
    through = jnp.exp(jnp.sum(fading_channel_groups, axis=0))

    def chain_states(earlier, later):
        return (earlier[0] * later[0], later[0][:, :, None] * earlier[1] + later[1])

    identity = (jnp.ones_like(through), jnp.zeros_like(nearby_hidden_vector))
    unused_decay, incoming_state = entering(
        (through, nearby_hidden_vector), "sp", chain_states, identity
    )
    running_sum = jnp.cumsum(fading_channel_groups, axis=0)
    recurrent = local_out + jnp.einsum(
        "fby,bym->fbm",
        query_rows_input * jnp.exp(running_sum),
        incoming_state,
        precision=lax.Precision.HIGHEST,
    )
    gated_out = head_norm(recurrent, recurrence_norm_gain.reshape(head_count, HEAD)) * jax.nn.silu(
        gate_b.astype(jnp.float32).reshape(tokens, head_count, HEAD)
    )
    mixed_b = gated_out.reshape(tokens, head_count * HEAD).astype(jnp.bfloat16)
    summed = lax.psum_scatter(
        (contract_rows(mixed_a, out_a) + contract_rows(mixed_b, out_b)).astype(jnp.bfloat16),
        "tp",
        scatter_dimension=0,
        tiled=True,
    )
    layer_out = summed[None]
    return (layer_out, row_log_total)


LEAF = 16
CHUNK = 128
TILE = 256
MESH = pl.DeviceIdType.MESH


def remote(src, dst, send, recv, **where):
    return pltpu.make_async_remote_copy(
        src_ref=src, dst_ref=dst, send_sem=send, recv_sem=recv, device_id=where, device_id_type=MESH
    )


def greet(peers):
    barrier = pltpu.get_barrier_semaphore()
    for where in peers:
        pl.semaphore_signal(barrier, inc=1, device_id=where, device_id_type=MESH)
    pl.semaphore_wait(barrier, len(peers))


def gather_kernel(
    n, x_ref, w_ref, e_ref, o_ref, X, W, E, O,
    x_send, x_recv, xx_send, xx_recv,
    w_send, w_recv, wy_send, wy_recv, wc_send, wc_recv, wd_send, wd_recv,
    e_send, e_recv,
    o_send, o_recv, oy_send, oy_recv, oc_send, oc_recv, od_send, od_recv,
    local_sem,
):
    z, f, x = lax.axis_index("sp"), lax.axis_index("fs"), lax.axis_index("tp")
    core, row, side = f + 1 - 2 * (f % 2), (f + 2) % 4, 1 - x
    half = x_ref.shape[0] // 2
    mine = pl.ds(pl.multiple_of(x * half, half), half)
    greet(
        [{"sp": (z + o) % n} for o in range(1, n)] + [{"fs": core}, {"fs": row}, {"tp": side}]
    )

    def reach(direction, k):
        if direction == 0:
            return (z - k >= 0) & (z + 1 < n), z - 1 - k >= 0, z - k, z - 1 - k, z + 1
        return (z + k < n) & (z - 1 >= 0), z + 1 + k < n, z + k, z + 1 + k, z - 1

    def x_copy(direction, k):
        _, _, out, _, to = reach(direction, k)
        src = x_ref.at[mine] if k == 0 else X.at[out, mine]
        return remote(src, X.at[out, mine], x_send.at[direction, k], x_recv.at[direction, k], sp=to)

    def xx_copy(direction, k):
        block = reach(direction, k)[3]
        return remote(X.at[block, mine], X.at[block, mine], xx_send.at[direction, k], xx_recv.at[direction, k], tp=side)

    def o_copy(direction, k):
        _, _, out, _, to = reach(direction, k)
        src = o_ref if k == 0 else O.at[out, f]
        return remote(src, O.at[out, f], o_send.at[direction, k], o_recv.at[direction, k], sp=to)

    def o_side(kind, direction, k):
        block = reach(direction, k)[3]
        if kind == 0:
            return remote(O.at[block, f], O.at[block, f], oy_send.at[direction, k], oy_recv.at[direction, k], fs=row)
        if kind == 1:
            return remote(O.at[block, f], O.at[block, f], oc_send.at[direction, k], oc_recv.at[direction, k], fs=core)
        return remote(O.at[block, row], O.at[block, row], od_send.at[direction, k], od_recv.at[direction, k], fs=core)

    def o_own(kind):
        if kind == 0:
            return remote(o_ref, O.at[z, f], oy_send.at[2, 0], oy_recv.at[2, 0], fs=row)
        if kind == 1:
            return remote(o_ref, O.at[z, f], oc_send.at[2, 0], oc_recv.at[2, 0], fs=core)
        return remote(O.at[z, row], O.at[z, row], od_send.at[2, 0], od_recv.at[2, 0], fs=core)

    def w_copy(o):
        return remote(w_ref.at[(z + o) % n], W.at[z, f], w_send.at[o], w_recv.at[o], sp=(z + o) % n)

    def e_copy(o):
        return remote(e_ref.at[(z + o) % n], E.at[z], e_send.at[o], e_recv.at[o], sp=(z + o) % n)

    def w_side(kind, o):
        block = (z - o + n) % n
        src = w_ref.at[z] if o == 0 else W.at[block, f]
        if kind == 0:
            return remote(src, W.at[block, f], wy_send.at[o], wy_recv.at[o], fs=row)
        if kind == 1:
            return remote(src, W.at[block, f], wc_send.at[o], wc_recv.at[o], fs=core)
        return remote(W.at[block, row], W.at[block, row], wd_send.at[o], wd_recv.at[o], fs=core)

    def sends(copy, direction, k):
        @pl.when(reach(direction, k)[0])
        def _():
            copy(direction, k).start()

    def received(direction, k, act):
        pl.when(reach(direction, k)[1])(act)

    both = (0, 1)
    for d in both:
        sends(x_copy, d, 0)
    local = [
        pltpu.make_async_copy(x_ref, X.at[z], local_sem.at[0]),
        pltpu.make_async_copy(w_ref.at[z], W.at[z, f], local_sem.at[1]),
        pltpu.make_async_copy(e_ref.at[z], E.at[z], local_sem.at[2]),
        pltpu.make_async_copy(o_ref, O.at[z, f], local_sem.at[3]),
    ]
    for copy in local:
        copy.start()
    for kind in both:
        w_side(kind, 0).start()
    for o in range(1, n):
        w_copy(o).start()
    for o in range(1, n):
        e_copy(o).start()
    for d in both:
        sends(o_copy, d, 0)
    for kind in both:
        o_own(kind).start()
    for k in range(n - 1):
        for d in both:
            def x_here(d=d, k=k):
                x_copy(d, k).wait_recv()
                xx_copy(d, k).start()
            received(d, k, x_here)
            if k + 1 < n - 1:
                sends(x_copy, d, k + 1)
        w_copy(k + 1).wait_recv()
        for kind in both:
            w_side(kind, k + 1).start()
        for d in both:
            def o_here(d=d, k=k):
                o_copy(d, k).wait_recv()
                for kind in both:
                    o_side(kind, d, k).start()
            received(d, k, o_here)
            if k + 1 < n - 1:
                sends(o_copy, d, k + 1)
    for o in range(n):
        w_side(0, o).wait_recv()
        w_side(2, o).start()
    o_own(0).wait_recv()
    o_own(2).start()
    for k in range(n - 1):
        for d in both:
            def o_next(d=d, k=k):
                o_side(0, d, k).wait_recv()
                o_side(2, d, k).start()
            received(d, k, o_next)
    for o in range(n):
        w_side(1, o).wait_recv()
        w_side(2, o).wait_recv()
        for kind in range(3):
            w_side(kind, o).wait_send()
    for o in range(1, n):
        e_copy(o).wait_recv()
        e_copy(o).wait_send()
        w_copy(o).wait_send()
    o_own(1).wait_recv()
    o_own(2).wait_recv()
    for kind in range(3):
        o_own(kind).wait_send()
    for k in range(n - 1):
        for d in both:
            def rest(d=d, k=k):
                xx_copy(d, k).wait_recv()
                xx_copy(d, k).wait_send()
                o_side(1, d, k).wait_recv()
                o_side(2, d, k).wait_recv()
                for kind in range(3):
                    o_side(kind, d, k).wait_send()
            received(d, k, rest)

            @pl.when(reach(d, k)[0])
            def _(d=d, k=k):
                x_copy(d, k).wait_send()
                o_copy(d, k).wait_send()
    for copy in local:
        copy.wait()


def nt_dot(a, b):
    return lax.dot_general(a, b, (((1,), (1,)), ((), ())), preferred_element_type=jnp.float32)


def tn_dot(a, b):
    return lax.dot_general(a, b, (((0,), (0,)), ((), ())), preferred_element_type=jnp.float32)


def grid_of(shape):
    return lax.broadcasted_iota(jnp.int32, shape, 0), lax.broadcasted_iota(jnp.int32, shape, 1)


def mixer_kernel(p_ref, e_ref, shift_ref, again_ref, rgain_ref, floor_ref, foff_ref, m_ref, keep_ref):
    rows = p_ref.shape[0]
    shift = shift_ref[...]
    r, c = grid_of((TILE, TILE))
    later = (r > c).astype(jnp.bfloat16)
    for i in range(rows // TILE):
        here = slice(i * TILE, (i + 1) * TILE)
        query = p_ref[here, 0:HEAD]
        total = jnp.zeros((TILE, HEAD), jnp.float32)
        keep = jnp.zeros((TILE, 1), jnp.float32)
        for j in range(i, -1, -1):
            there = slice(j * TILE, (j + 1) * TILE)
            score = nt_dot(query, p_ref[there, HEAD : 2 * HEAD]) * HEAD ** (-0.5) + shift
            soft = -(jnp.maximum(score, 0.0) + jnp.log1p(jnp.exp(-jnp.abs(score))))
            held = jnp.where(r > c, soft, 0.0) if i == j else soft
            high = held.astype(jnp.bfloat16)
            low = (held - high.astype(jnp.float32)).astype(jnp.bfloat16)
            suffix = jnp.dot(high, later, preferred_element_type=jnp.float32) + jnp.dot(
                low, later, preferred_element_type=jnp.float32
            )
            weight = jnp.exp(score + soft + suffix + keep)
            if i == j:
                weight = jnp.where(r > c, weight, 0.0)
            total += jnp.dot(
                weight.astype(jnp.bfloat16),
                p_ref[there, 2 * HEAD : 3 * HEAD],
                preferred_element_type=jnp.float32,
            )
            keep += jnp.sum(held, axis=1, keepdims=True)
        m_ref[here, 0:HEAD] = head_norm(total, again_ref[...]).astype(jnp.bfloat16)
        keep_ref[here, :] = keep

    floor, offset, gain = floor_ref[...], foff_ref[...], rgain_ref[...]
    r, c = grid_of((CHUNK, CHUNK))
    lower = (r >= c).astype(jnp.float32)

    def chunk(i, state):
        here = pl.ds(pl.multiple_of(i * CHUNK, CHUNK), CHUNK)
        part = lambda k: p_ref[here, k * HEAD : (k + 1) * HEAD].astype(jnp.float32)
        raw = part(3)
        query = raw * jax.nn.sigmoid(raw)
        key = (1.0 - floor) * jax.nn.sigmoid(-(part(4) + offset))
        value = p_ref[here, 5 * HEAD : 6 * HEAD]
        gate = part(6)
        decay = jnp.log1p(-key) + e_ref[here, :].astype(jnp.float32)
        run = jnp.dot(lower, decay, precision=lax.Precision.HIGHEST, preferred_element_type=jnp.float32)
        stripes = [jnp.zeros((LEAF, CHUNK), jnp.float32)]
        for s in range(LEAF, CHUNK, LEAF):
            edge = run[s - 1 : s, :]
            near = (query[s : s + LEAF] * jnp.exp(run[s : s + LEAF] - edge)).astype(jnp.bfloat16)
            far = (key * jnp.exp(jnp.where(r < s, edge - run, -jnp.inf))).astype(jnp.bfloat16)
            stripes.append(nt_dot(near, far))
        pairs = jnp.concatenate(stripes, axis=0)
        for d in range(LEAF):
            back_key = pltpu.roll(key, d, 0) if d else key
            back_run = pltpu.roll(run, d, 0) if d else run
            gap = jnp.where(r % LEAF >= d, run - back_run, -jnp.inf)
            column = jnp.sum(query * back_key * jnp.exp(gap), axis=1, keepdims=True)
            pairs = jnp.where((r - c == d) & (r % LEAF >= d), column, pairs)
        last = run[CHUNK - 1 : CHUNK, :]
        out = jnp.dot(pairs.astype(jnp.bfloat16), value, preferred_element_type=jnp.float32)
        out += nt_dot((query * jnp.exp(run)).astype(jnp.bfloat16), state.astype(jnp.bfloat16))
        mixed = head_norm(out, gain) * (gate * jax.nn.sigmoid(gate))
        m_ref[here, HEAD : 2 * HEAD] = mixed.astype(jnp.bfloat16)
        return jnp.exp(last) * state + tn_dot(value, (key * jnp.exp(last - run)).astype(jnp.bfloat16))

    lax.fori_loop(0, rows // CHUNK, chunk, jnp.zeros((HEAD, HEAD), jnp.float32))


PIECES = 4


def output_kernel(
    n, m_ref, t_ref, o_ref, out_ref, T, M, away, landed,
    m_send, m_recv, t_send, t_recv, y_send, y_recv, local_sem,
):
    z, x = lax.axis_index("sp"), lax.axis_index("tp")
    side = 1 - x
    half = out_ref.shape[0]
    greet([{"sp": (z + o) % n} for o in range(1, n)] + [{"tp": side}])

    def m_copy(o):
        return remote(m_ref.at[(z + o) % n], M.at[z], m_send.at[o], m_recv.at[o], sp=(z + o) % n)

    def t_copy(o):
        return remote(t_ref.at[(z + o) % n], T.at[z], t_send.at[o], t_recv.at[o], sp=(z + o) % n)

    for o in range(1, n):
        m_copy(o).start()
    for o in range(1, n):
        t_copy(o).start()
    local = [
        pltpu.make_async_copy(m_ref.at[z], M.at[z], local_sem.at[0]),
        pltpu.make_async_copy(t_ref.at[z], T.at[z], local_sem.at[1]),
    ]
    for copy in local:
        copy.start()
    for copy in local:
        copy.wait()
    for o in range(1, n):
        m_copy(o).wait()

    def rows_of(which):
        rows = pl.ds(pl.multiple_of(which * half, half), half)
        parts = [M[k, rows, g * HEAD : (g + 1) * HEAD] for g in (0, 1) for k in range(n)]
        return jnp.concatenate(parts, axis=1)

    width = out_ref.shape[1] // PIECES

    def y_copy(j):
        return remote(away.at[j], landed.at[j], y_send.at[j], y_recv.at[j], tp=side)

    theirs = rows_of(side)
    for j in range(PIECES):
        away[j] = nt_dot(theirs, o_ref[j * width : (j + 1) * width, :]).astype(jnp.bfloat16)
        if j:
            y_copy(j - 1).start()
    ours = rows_of(x)
    for j in range(PIECES):
        piece = nt_dot(ours, o_ref[j * width : (j + 1) * width, :])
        if j == 0:
            y_copy(PIECES - 1).start()
        y_copy(j).wait_recv()
        piece += landed[j].astype(jnp.float32)
        out_ref[:, j * width : (j + 1) * width] = piece.astype(jnp.bfloat16)
    for j in range(PIECES):
        y_copy(j).wait_send()
    for o in range(1, n):
        t_copy(o).wait()


VMEM = pl.BlockSpec(memory_space=pltpu.VMEM)
DMA = pltpu.SemaphoreType.DMA


def on_device_heads(
    n,
    input_layer_rows,
    input_norm_gain,
    query_weight_attention,
    key_weight_attention,
    value_weight_attention,
    query_weight_recurrent,
    forget_weight_recurrent,
    value_weight_recurrent,
    gate_weight_recurrent,
    output_weight_attention,
    emitted_projection_linear_scan,
    score_offset,
    attention_norm_gain,
    recurrence_norm_gain,
    forget_floor,
    forget_offset,
    extra_log_decay,
):
    values = input_layer_rows[0].astype(jnp.float32)
    square_mean = jnp.mean(values * values, axis=-1, keepdims=True)
    normed = (values * lax.rsqrt(square_mean + epsilon) * input_norm_gain).astype(jnp.bfloat16)
    tokens, depth = normed.shape
    groups = lax.axis_size("fs")
    weights_in = (
        query_weight_attention,
        key_weight_attention,
        value_weight_attention,
        query_weight_recurrent,
        forget_weight_recurrent,
        value_weight_recurrent,
        gate_weight_recurrent,
    )
    share = weights_in[0].shape[0]
    width = len(weights_in) * HEAD
    by_head = jnp.stack(
        [
            jnp.concatenate([w[:, h * HEAD : (h + 1) * HEAD] for w in weights_in], axis=1)
            for h in range(n)
        ]
    )
    extra = extra_log_decay[0].astype(jnp.bfloat16)
    extra = jnp.stack([extra[:, h * HEAD : (h + 1) * HEAD] for h in range(n)])
    both_out = jnp.concatenate([output_weight_attention, emitted_projection_linear_scan], axis=1)
    X, W, E, O = pl.pallas_call(
        functools.partial(gather_kernel, n),
        out_shape=(
            jax.ShapeDtypeStruct((n, tokens, depth), jnp.bfloat16),
            jax.ShapeDtypeStruct((n, groups, share, width), jnp.bfloat16),
            jax.ShapeDtypeStruct((n, tokens, HEAD), jnp.bfloat16),
            jax.ShapeDtypeStruct((n, groups, share, both_out.shape[1]), jnp.bfloat16),
        ),
        in_specs=[VMEM] * 4,
        out_specs=(VMEM,) * 4,
        scratch_shapes=[DMA((2, n))] * 4 + [DMA((n,))] * 10 + [DMA((2, n))] * 2 + [DMA((3, n))] * 6 + [DMA((4,))],
        compiler_params=pltpu.CompilerParams(
            collective_id=0, has_side_effects=True, vmem_limit_bytes=50 * 1024 * 1024
        ),
    )(normed, by_head, extra, both_out)
    projected = jnp.dot(
        X.reshape(n * tokens, depth), W.reshape(depth, width), preferred_element_type=jnp.float32
    ).astype(jnp.bfloat16)
    z = lax.axis_index("sp")
    own = lambda a: lax.dynamic_slice_in_dim(a, z * HEAD, HEAD)[None]
    mixed, keep = pl.pallas_call(
        mixer_kernel,
        out_shape=(
            jax.ShapeDtypeStruct((n * tokens, 2 * HEAD), jnp.bfloat16),
            jax.ShapeDtypeStruct((n * tokens, 1), jnp.float32),
        ),
        in_specs=[VMEM] * 7,
        out_specs=(VMEM,) * 2,
        compiler_params=pltpu.CompilerParams(vmem_limit_bytes=40 * 1024 * 1024),
    )(
        projected,
        E.reshape(n * tokens, HEAD),
        lax.dynamic_slice_in_dim(score_offset, z, 1)[None],
        own(attention_norm_gain),
        own(recurrence_norm_gain),
        own(forget_floor),
        own(forget_offset),
    )
    totals = jnp.log(jnp.maximum(-jnp.expm1(keep[:, 0]), log_floor)).reshape(n, 1, tokens)
    totals = jnp.broadcast_to(totals, (n, 8, tokens))
    half = tokens // 2
    layer_out, T = pl.pallas_call(
        functools.partial(output_kernel, n),
        out_shape=(
            jax.ShapeDtypeStruct((half, depth), jnp.bfloat16),
            jax.ShapeDtypeStruct((n, 8, tokens), jnp.float32),
        ),
        in_specs=[VMEM] * 3,
        out_specs=(VMEM,) * 2,
        scratch_shapes=[
            pltpu.VMEM((n, tokens, 2 * HEAD), jnp.bfloat16),
            pltpu.VMEM((PIECES, half, depth // PIECES), jnp.bfloat16),
            pltpu.VMEM((PIECES, half, depth // PIECES), jnp.bfloat16),
        ]
        + [DMA((n,))] * 4
        + [DMA((PIECES,))] * 2
        + [DMA((2,))],
        compiler_params=pltpu.CompilerParams(
            collective_id=1, has_side_effects=True, vmem_limit_bytes=40 * 1024 * 1024
        ),
    )(mixed.reshape(n, tokens, 2 * HEAD), totals, O.reshape(depth, both_out.shape[1]))
    return (layer_out[None], T[:, 0, :][None])


def solution(mesh):
    n = mesh.shape["sp"]
    heads_fit = mesh.shape["fs"] == 4 and mesh.shape["tp"] == 2 and n > 1

    def on_device(*args):
        if heads_fit and args[11].shape[0] == n and args[0].shape[1] % TILE == 0:
            return on_device_heads(n, *args)
        return on_device_general(*args)

    return jax.shard_map(
        on_device,
        mesh=mesh,
        in_specs=(
            P("fs", "sp", None),
            P(),
            P(("sp", "fs"), "tp"),
            P(("sp", "fs"), "tp"),
            P(("sp", "fs"), "tp"),
            P(("sp", "fs"), "tp"),
            P(("sp", "fs"), "tp"),
            P(("sp", "fs"), "tp"),
            P(("sp", "fs"), "tp"),
            P(("sp", "fs"), "tp"),
            P(("sp", "fs"), "tp"),
            P("tp"),
            P("tp"),
            P("tp"),
            P("tp"),
            P("tp"),
            P("fs", "sp", "tp"),
        ),
        out_specs=(P("fs", ("sp", "tp"), None), P("fs", "tp", "sp")),
        check_vma=False,
    )
```

```python
import functools
import jax
import jax.numpy as jnp
from jax import lax
from jax.experimental import pallas as pl
from jax.experimental.pallas import tpu as pltpu
from jax.sharding import PartitionSpec as P

HEAD = 128
BLOCK = 64


epsilon = 1e-06
log_floor = 0.05


def entering(shard, axis, combine, identity):
    size, index = (lax.axis_size(axis), lax.axis_index(axis))
    everything = jax.tree.map(
        lambda part, kind: lax.all_gather(part.astype(kind), axis),
        shard,
        (jnp.bfloat16, jnp.bfloat16),
    )
    start = jax.tree.map(
        lambda part, zero: jnp.broadcast_to(jnp.asarray(zero, part.dtype), part.shape),
        shard,
        identity,
    )

    def hop(k, before):
        reached = k < index
        new = combine(
            before, jax.tree.map(lambda part, own: part[k].astype(own.dtype), everything, shard)
        )
        return jax.tree.map(lambda a, b: jnp.where(reached, a, b), new, before)

    return lax.fori_loop(0, size, hop, start)


def head_norm(values, gain):
    square_mean = jnp.mean(values * values, axis=-1, keepdims=True)
    return values * lax.rsqrt(square_mean + epsilon) * gain


def recurrence_block(memory_matrix, inputs):
    query_slice, decay_part, key_slice, value_slice = inputs
    highest_score = lax.Precision.HIGHEST
    length = decay_part.shape[0]
    running_total = jnp.cumsum(decay_part, axis=0)
    causal = (
        lax.broadcasted_iota(jnp.int32, (length, length), 0)
        >= lax.broadcasted_iota(jnp.int32, (length, length), 1)
    )[:, :, None, None]
    relative = jnp.where(causal, running_total[:, None] - running_total[None, :], -jnp.inf)
    pairwise = jnp.sum(query_slice[:, None] * key_slice[None, :] * jnp.exp(relative), axis=-1)
    inner_part = jnp.einsum("tsh,shv->thv", pairwise, value_slice, precision=highest_score)
    carried_state = jnp.einsum(
        "fby,bym->fbm", query_slice * jnp.exp(running_total), memory_matrix, precision=highest_score
    )
    final_total = running_total[-1]
    updated_state = jnp.exp(final_total)[:, :, None] * memory_matrix + jnp.einsum(
        "rxc,rxa->xca",
        key_slice * jnp.exp(final_total[None] - running_total),
        value_slice,
        precision=highest_score,
    )
    return (updated_state, inner_part + carried_state)


def stick_piece(queries, shifts, weighted, keep_total, key_value, is_own, is_valid):
    scores = (
        jnp.einsum("thd,shd->hts", queries, key_value[0], preferred_element_type=jnp.float32)
        * HEAD ** (-0.5)
        + shifts[:, None, None]
    )
    logarithmic_retention = jax.nn.log_sigmoid(-scores)
    if is_own:
        rows_here = scores.shape[1]
        strict = lax.broadcasted_iota(jnp.int32, (rows_here, rows_here), 0) > lax.broadcasted_iota(
            jnp.int32, (rows_here, rows_here), 1
        )
        logarithmic_retention = jnp.where(strict, logarithmic_retention, 0.0)
    suffix = lax.cumsum(logarithmic_retention, axis=2, reverse=True) - logarithmic_retention
    log_weight = jax.nn.log_sigmoid(scores) + suffix + keep_total[:, :, None]
    if is_own:
        log_weight = jnp.where(strict, log_weight, -jnp.inf)
    weights = jnp.where(is_valid, jnp.exp(log_weight), 0.0).astype(jnp.bfloat16)
    weighted = weighted + jnp.einsum(
        "hts,shd->thd", weights, key_value[1], preferred_element_type=jnp.float32
    )
    keep_total = keep_total + jnp.where(is_valid, jnp.sum(logarithmic_retention, axis=2), 0.0)
    return (weighted, keep_total)


def contract_rows(rows_in, weight):
    return lax.dot_general(
        rows_in, weight, (((1,), (1,)), ((), ())), preferred_element_type=jnp.float32
    )


def on_device_general(
    input_layer_rows,
    input_norm_gain,
    query_weight_attention,
    key_weight_attention,
    value_weight_attention,
    query_weight_recurrent,
    forget_weight_recurrent,
    value_weight_recurrent,
    gate_weight_recurrent,
    output_weight_attention,
    emitted_projection_linear_scan,
    score_offset,
    attention_norm_gain,
    recurrence_norm_gain,
    forget_floor,
    forget_offset,
    extra_log_decay,
):
    values = input_layer_rows[0].astype(jnp.float32)
    square_mean = jnp.mean(values * values, axis=-1, keepdims=True)
    normed = (values * lax.rsqrt(square_mean + epsilon) * input_norm_gain).astype(jnp.bfloat16)
    tokens = normed.shape[0]
    weights_in = (
        query_weight_attention,
        key_weight_attention,
        value_weight_attention,
        query_weight_recurrent,
        forget_weight_recurrent,
        value_weight_recurrent,
        gate_weight_recurrent,
    )
    pieces = (
        lax.all_gather(weights_in[0], ("sp", "fs"), axis=0, tiled=True),
        lax.all_gather(weights_in[1], ("sp", "fs"), axis=0, tiled=True),
        lax.all_gather(weights_in[2], ("sp", "fs"), axis=0, tiled=True),
        lax.all_gather(weights_in[3], ("sp", "fs"), axis=0, tiled=True),
        lax.all_gather(weights_in[4], ("sp", "fs"), axis=0, tiled=True),
        lax.all_gather(weights_in[5], ("sp", "fs"), axis=0, tiled=True),
        lax.all_gather(weights_in[6], ("sp", "fs"), axis=0, tiled=True),
    )
    projected = tuple(
        (jnp.dot(normed, weight, preferred_element_type=jnp.float32) for weight in pieces)
    )
    query_a, key_a, value_a, query_b, forget_b, input_b, gate_b = [
        column_block.astype(jnp.bfloat16) for column_block in projected
    ]
    out_a, out_b = (
        lax.all_gather(output_weight_attention, ("sp", "fs"), axis=0, tiled=True),
        lax.all_gather(emitted_projection_linear_scan, ("sp", "fs"), axis=0, tiled=True),
    )
    head_count = query_a.shape[1] // HEAD
    queries = query_a.reshape(tokens, head_count, HEAD)
    key_value = jnp.stack(
        [key_a.reshape(tokens, head_count, HEAD), value_a.reshape(tokens, head_count, HEAD)]
    )
    weighted = jnp.zeros((tokens, head_count, HEAD), jnp.float32)
    keep_total = jnp.zeros((head_count, tokens), jnp.float32)
    weighted, keep_total = stick_piece(
        queries, score_offset, weighted, keep_total, key_value, True, True
    )
    position = lax.axis_index("sp")
    seq_devices = lax.axis_size("sp")
    gathered = lax.all_gather(key_value, "sp", axis=1, tiled=True)

    def gathered_turn(turn_index, carried_state):
        weighted_now, keep_now = carried_state
        source = jnp.maximum(position - turn_index, 0) * tokens
        piece_pair = lax.dynamic_slice_in_dim(gathered, source, tokens, 1)
        return stick_piece(
            queries, score_offset, weighted_now, keep_now, piece_pair, False, position >= turn_index
        )

    weighted, keep_total = lax.fori_loop(1, seq_devices, gathered_turn, (weighted, keep_total))
    row_log_total = jnp.log(jnp.maximum(-jnp.expm1(keep_total), log_floor))[None]
    mixed_a = (
        head_norm(weighted, attention_norm_gain.reshape(head_count, HEAD))
        .reshape(tokens, head_count * HEAD)
        .astype(jnp.bfloat16)
    )
    forget_logits = forget_b.astype(jnp.float32) + forget_offset
    forget_log_value = (
        jnp.logaddexp(
            jnp.log(forget_floor), jnp.log1p(-forget_floor) + jax.nn.log_sigmoid(forget_logits)
        )
        + extra_log_decay[0]
    )
    key_in = (1.0 - forget_floor) * jax.nn.sigmoid(-forget_logits)
    query_rows_input = jax.nn.silu(query_b.astype(jnp.float32)).reshape(tokens, head_count, HEAD)
    value_in = input_b.astype(jnp.float32)
    fading_channel_groups = forget_log_value.reshape(tokens, head_count, HEAD)
    shaped = tuple(
        (
            array_in.reshape(tokens // BLOCK, BLOCK, head_count, HEAD)
            for array_in in (query_rows_input, forget_log_value, key_in, value_in)
        )
    )
    empty_state = jnp.zeros((head_count, HEAD, HEAD), jnp.float32)
    nearby_hidden_vector, local_out = lax.scan(recurrence_block, empty_state, shaped)
    local_out = local_out.reshape(tokens, head_count, HEAD)
    through = jnp.exp(jnp.sum(fading_channel_groups, axis=0))

    def chain_states(earlier, later):
        return (earlier[0] * later[0], later[0][:, :, None] * earlier[1] + later[1])

    identity = (jnp.ones_like(through), jnp.zeros_like(nearby_hidden_vector))
    unused_decay, incoming_state = entering(
        (through, nearby_hidden_vector), "sp", chain_states, identity
    )
    running_sum = jnp.cumsum(fading_channel_groups, axis=0)
    recurrent = local_out + jnp.einsum(
        "fby,bym->fbm",
        query_rows_input * jnp.exp(running_sum),
        incoming_state,
        precision=lax.Precision.HIGHEST,
    )
    gated_out = head_norm(recurrent, recurrence_norm_gain.reshape(head_count, HEAD)) * jax.nn.silu(
        gate_b.astype(jnp.float32).reshape(tokens, head_count, HEAD)
    )
    mixed_b = gated_out.reshape(tokens, head_count * HEAD).astype(jnp.bfloat16)
    summed = lax.psum_scatter(
        (contract_rows(mixed_a, out_a) + contract_rows(mixed_b, out_b)).astype(jnp.bfloat16),
        "tp",
        scatter_dimension=0,
        tiled=True,
    )
    layer_out = summed[None]
    return (layer_out, row_log_total)


LEAF = 16
CHUNK = 128
TILE = 256
MESH = pl.DeviceIdType.MESH


def remote(src, dst, send, recv, **where):
    return pltpu.make_async_remote_copy(
        src_ref=src, dst_ref=dst, send_sem=send, recv_sem=recv, device_id=where, device_id_type=MESH
    )


def greet(peers):
    barrier = pltpu.get_barrier_semaphore()
    for where in peers:
        pl.semaphore_signal(barrier, inc=1, device_id=where, device_id_type=MESH)
    pl.semaphore_wait(barrier, len(peers))


def nt_dot(a, b):
    return lax.dot_general(a, b, (((1,), (1,)), ((), ())), preferred_element_type=jnp.float32)


def tn_dot(a, b):
    return lax.dot_general(a, b, (((0,), (0,)), ((), ())), preferred_element_type=jnp.float32)


def grid_of(shape):
    return lax.broadcasted_iota(jnp.int32, shape, 0), lax.broadcasted_iota(jnp.int32, shape, 1)


def attend_tile(i, p_ref, shift, gain):
    here = slice(i * TILE, (i + 1) * TILE)
    r, c = grid_of((TILE, TILE))
    later = (r > c).astype(jnp.bfloat16)
    query = p_ref[here, 0:HEAD]
    total = jnp.zeros((TILE, HEAD), jnp.float32)
    keep = jnp.zeros((TILE, 1), jnp.float32)
    for j in range(i, -1, -1):
        there = slice(j * TILE, (j + 1) * TILE)
        score = nt_dot(query, p_ref[there, HEAD : 2 * HEAD]) * HEAD ** (-0.5) + shift
        soft = -(jnp.maximum(score, 0.0) + jnp.log1p(jnp.exp(-jnp.abs(score))))
        held = jnp.where(r > c, soft, 0.0) if i == j else soft
        high = held.astype(jnp.bfloat16)
        low = (held - high.astype(jnp.float32)).astype(jnp.bfloat16)
        suffix = jnp.dot(high, later, preferred_element_type=jnp.float32) + jnp.dot(
            low, later, preferred_element_type=jnp.float32
        )
        weight = jnp.exp(score + soft + suffix + keep)
        if i == j:
            weight = jnp.where(r > c, weight, 0.0)
        total += jnp.dot(
            weight.astype(jnp.bfloat16),
            p_ref[there, 2 * HEAD : 3 * HEAD],
            preferred_element_type=jnp.float32,
        )
        keep += jnp.sum(held, axis=1, keepdims=True)
    return head_norm(total, gain).astype(jnp.bfloat16), keep


def recur_chunk(p_ref, e_ref, here, state, floor, offset, gain):
    r, c = grid_of((CHUNK, CHUNK))
    lower = (r >= c).astype(jnp.float32)
    part = lambda k: p_ref[here, k * HEAD : (k + 1) * HEAD].astype(jnp.float32)
    raw = part(3)
    query = raw * jax.nn.sigmoid(raw)
    key = (1.0 - floor) * jax.nn.sigmoid(-(part(4) + offset))
    value = p_ref[here, 5 * HEAD : 6 * HEAD]
    gate = part(6)
    decay = jnp.log1p(-key) + e_ref[...].astype(jnp.float32)
    run = jnp.dot(lower, decay, precision=lax.Precision.HIGHEST, preferred_element_type=jnp.float32)
    stripes = [jnp.zeros((LEAF, CHUNK), jnp.float32)]
    for s in range(LEAF, CHUNK, LEAF):
        edge = run[s - 1 : s, :]
        near = (query[s : s + LEAF] * jnp.exp(run[s : s + LEAF] - edge)).astype(jnp.bfloat16)
        far = (key * jnp.exp(jnp.where(r < s, edge - run, -jnp.inf))).astype(jnp.bfloat16)
        stripes.append(nt_dot(near, far))
    pairs = jnp.concatenate(stripes, axis=0)
    for d in range(LEAF):
        back_key = pltpu.roll(key, d, 0) if d else key
        back_run = pltpu.roll(run, d, 0) if d else run
        gap = jnp.where(r % LEAF >= d, run - back_run, -jnp.inf)
        column = jnp.sum(query * back_key * jnp.exp(gap), axis=1, keepdims=True)
        pairs = jnp.where((r - c == d) & (r % LEAF >= d), column, pairs)
    last = run[CHUNK - 1 : CHUNK, :]
    out = jnp.dot(pairs.astype(jnp.bfloat16), value, preferred_element_type=jnp.float32)
    out += nt_dot((query * jnp.exp(run)).astype(jnp.bfloat16), state.astype(jnp.bfloat16))
    mixed = head_norm(out, gain) * (gate * jax.nn.sigmoid(gate))
    state = jnp.exp(last) * state + tn_dot(value, (key * jnp.exp(last - run)).astype(jnp.bfloat16))
    return mixed.astype(jnp.bfloat16), state


PARTS = 2


def layer_kernel(n, *refs):
    x_ref, e_ref, v_ref = refs[:3]
    w_refs, o_refs = refs[3:10], refs[10:12]
    out_ref, T = refs[12:14]
    (
        X, W, O, E, wp, proj, ma, mb, ts, M, away, landed,
        x_send, x_recv, xx_send, xx_recv,
        o_send, o_recv, oy_send, oy_recv, oc_send, oc_recv, od_send, od_recv,
        w_send, w_recv, wy_send, wy_recv, wc_send, wc_recv, wd_send, wd_recv,
        e_send, e_recv, m_send, m_recv, b_send, b_recv, t_send, t_recv, y_send, y_recv,
        pack_sem, local_sem,
    ) = refs[14:]
    z, f, x = lax.axis_index("sp"), lax.axis_index("fs"), lax.axis_index("tp")
    core, row, side = f + 1 - 2 * (f % 2), (f + 2) % 4, 1 - x
    tokens = x_ref.shape[0]
    half = tokens // 2
    step = half // PARTS
    both = (0, 1)

    def cols(h):
        return pl.ds(pl.multiple_of(h * HEAD, HEAD), HEAD)

    packs = []
    for i, w in enumerate(w_refs):
        for h in range(n):
            packs.append(
                pltpu.make_async_copy(
                    w.at[:, h * HEAD : (h + 1) * HEAD],
                    wp.at[h, :, i * HEAD : (i + 1) * HEAD],
                    pack_sem.at[i, h],
                )
            )
    wide = o_refs[0].shape[1]
    for i, o in enumerate(o_refs):
        packs.append(
            pltpu.make_async_copy(o, O.at[z, f, :, i * wide : (i + 1) * wide], local_sem.at[i])
        )
    for copy in packs:
        copy.start()
    local = [
        pltpu.make_async_copy(x_ref, X.at[z], local_sem.at[2]),
        pltpu.make_async_copy(e_ref.at[:, cols(z)], E.at[z], local_sem.at[3]),
    ]
    for copy in local:
        copy.start()
    greet(
        [{"sp": (z + o) % n} for o in range(1, n)] + [{"fs": core}, {"fs": row}, {"tp": side}]
    )

    def reach(direction, k):
        if direction == 0:
            return (z - k >= 0) & (z + 1 < n), z - 1 - k >= 0, z - k, z - 1 - k, z + 1
        return (z + k < n) & (z - 1 >= 0), z + 1 + k < n, z + k, z + 1 + k, z - 1

    def span(c):
        return pl.ds(pl.multiple_of(x * half + c * step, step), step)

    def x_copy(direction, k, c, first=False):
        _, _, out, _, to = reach(direction, k)
        src = x_ref.at[span(c)] if first else X.at[out, span(c)]
        return remote(
            src, X.at[out, span(c)], x_send.at[direction, k, c], x_recv.at[direction, k, c], sp=to
        )

    def x_wait(direction, k, c):
        block = X.at[reach(direction, k)[3], span(c)]
        return remote(block, block, x_send.at[direction, k, c], x_recv.at[direction, k, c], sp=(z + 1) % n)

    def xx_copy(direction, k, c):
        block = X.at[reach(direction, k)[3], span(c)]
        return remote(block, block, xx_send.at[direction, k, c], xx_recv.at[direction, k, c], tp=side)

    def xx_wait(direction, k, c):
        there = pl.ds(pl.multiple_of(side * half + c * step, step), step)
        block = X.at[reach(direction, k)[3], there]
        return remote(block, block, xx_send.at[direction, k, c], xx_recv.at[direction, k, c], tp=side)

    def o_copy(direction, k):
        _, _, out, _, to = reach(direction, k)
        return remote(O.at[out, f], O.at[out, f], o_send.at[direction, k], o_recv.at[direction, k], sp=to)

    def o_side(kind, direction, k, own=False):
        block = z if own else reach(direction, k)[3]
        send, recv = ((oy_send, oy_recv), (oc_send, oc_recv), (od_send, od_recv))[kind]
        piece = O.at[block, row if kind == 2 else f]
        where = {"fs": row if kind == 0 else core}
        return remote(piece, piece, send.at[direction, k], recv.at[direction, k], **where)

    def o_own(kind):
        return o_side(kind, 2, 0, own=True)

    def w_copy(o):
        return remote(wp.at[(z + o) % n], W.at[z, f], w_send.at[o], w_recv.at[o], sp=(z + o) % n)

    def e_copy(o):
        return remote(e_ref.at[:, cols((z + o) % n)], E.at[z], e_send.at[o], e_recv.at[o], sp=(z + o) % n)

    def w_side(kind, o):
        block = (z - o + n) % n
        src = wp.at[z] if o == 0 else W.at[block, f]
        if kind == 0:
            return remote(src, W.at[block, f], wy_send.at[o], wy_recv.at[o], fs=row)
        if kind == 1:
            return remote(src, W.at[block, f], wc_send.at[o], wc_recv.at[o], fs=core)
        return remote(W.at[block, row], W.at[block, row], wd_send.at[o], wd_recv.at[o], fs=core)

    for copy in packs:
        copy.wait()
    own_w = pltpu.make_async_copy(wp.at[z], W.at[z, f], local_sem.at[4])
    own_w.start()
    for o in range(1, n):
        w_copy(o).start()
    for kind in both:
        w_side(kind, 0).start()
    for d in both:
        @pl.when(reach(d, 0)[0])
        def _(d=d):
            for c in range(PARTS):
                x_copy(d, 0, c, True).start()
    for o in range(1, n):
        e_copy(o).start()
    for o in range(1, n):
        w_copy(o).wait_recv()
        for kind in both:
            w_side(kind, o).start()
    for kind in both:
        o_own(kind).start()
    for copy in local:
        copy.wait()
    own_w.wait()

    def project(block):
        rows = X[block]
        weights = W[...].reshape(rows.shape[1], W.shape[3])
        made = jnp.dot(rows, weights, preferred_element_type=jnp.float32)
        at = pl.ds(pl.multiple_of(block * tokens, tokens), tokens)
        proj[at, :] = made.astype(jnp.bfloat16)

    def gather_step(k, carry):
        for d in both:
            @pl.when((k < n - 1) & reach(d, k)[1])
            def _(d=d):
                for c in range(PARTS):
                    x_wait(d, k, c).wait_recv()

                    @pl.when(reach(d, k + 1)[0])
                    def _(c=c):
                        x_copy(d, k + 1, c).start()
                    xx_copy(d, k, c).start()

        @pl.when(k == max(n - 3, 0))
        def _():
            for d in both:
                @pl.when(reach(d, 0)[0])
                def _(d=d):
                    o_copy(d, 0).start()

        @pl.when(k == 0)
        def _():
            for o in range(n):
                w_side(0, o).wait_recv()
                w_side(2, o).start()
            for o in range(n):
                w_side(1, o).wait_recv()
                w_side(2, o).wait_recv()

        @pl.when(z - k >= 0)
        def _():
            @pl.when(k > 0)
            def _():
                for c in range(PARTS):
                    xx_wait(0, k - 1, c).wait_recv()
            project(z - k)

        @pl.when((k > 0) & (z + k < n))
        def _():
            for c in range(PARTS):
                xx_wait(1, k - 1, c).wait_recv()
            project(z + k)
        return carry

    lax.fori_loop(0, n, gather_step, 0)

    def o_tick(k):
        for d in both:
            @pl.when(reach(d, k)[1])
            def _(d=d):
                o_copy_in = O.at[reach(d, k)[3], f]
                remote(o_copy_in, o_copy_in, o_send.at[d, k], o_recv.at[d, k], sp=(z + 1) % n).wait_recv()
                if k + 1 < n - 1:
                    @pl.when(reach(d, k + 1)[0])
                    def _():
                        o_copy(d, k + 1).start()
                for kind in both:
                    o_side(kind, d, k).start()

    def m_copy(o):
        return remote(ma.at[(z + o) % n], M.at[0, z], m_send.at[o], m_recv.at[o], sp=(z + o) % n)

    def b_copy(o):
        return remote(mb.at[(z + o) % n], M.at[1, z], b_send.at[o], b_recv.at[o], sp=(z + o) % n)

    def t_copy(o):
        return remote(ts.at[(z + o) % n], T.at[z], t_send.at[o], t_recv.at[o], sp=(z + o) % n)

    param = lambda i: v_ref[i, pl.ds(z, 1), :]
    shift = param(0)[:, 0:1]
    for i in range(n):
        mixed, keep = attend_tile(i, proj, shift, param(1))
        ma[i] = mixed
        total = jnp.log(jnp.maximum(1.0 - jnp.exp(keep), log_floor))
        ts[i] = jnp.broadcast_to(total, (tokens, HEAD)).T[0:8, :]
    o_tick(0)
    for o in range(1, n):
        e_copy(o).wait_recv()
    floor, offset, gain = param(3), param(4), param(2)
    per = tokens // CHUNK

    def chunk(i, state):
        here = pl.ds(pl.multiple_of(i * CHUNK, CHUNK), CHUNK)
        at = pl.ds(pl.multiple_of((i % per) * CHUNK, CHUNK), CHUNK)
        extra = E.at[i // per, at]
        mixed, state = recur_chunk(proj, extra, here, state, floor, offset, gain)
        mb[i // per, at, :] = mixed
        return state

    state = jnp.zeros((HEAD, HEAD), jnp.float32)
    state = lax.fori_loop(0, per * n // 2, chunk, state)
    for o in range(1, n):
        m_copy(o).start()
    for o in range(1, n):
        t_copy(o).start()
    if n > 2:
        o_tick(1)
    lax.fori_loop(per * n // 2, per * n, chunk, state)
    for k in range(2, n - 1):
        o_tick(k)
    mine = [
        pltpu.make_async_copy(ma.at[z], M.at[0, z], local_sem.at[5]),
        pltpu.make_async_copy(mb.at[z], M.at[1, z], local_sem.at[6]),
        pltpu.make_async_copy(ts.at[z], T.at[z], local_sem.at[7]),
    ]
    for o in range(1, n):
        b_copy(o).start()
    for copy in mine:
        copy.start()
    o_own(0).wait_recv()
    o_own(2).start()
    for k in range(n - 1):
        for d in both:
            @pl.when(reach(d, k)[1])
            def _(d=d, k=k):
                o_side(0, d, k).wait_recv()
                o_side(2, d, k).start()
    for copy in mine:
        copy.wait()
    for o in range(1, n):
        m_copy(o).wait()
        b_copy(o).wait()
    o_own(1).wait_recv()
    o_own(2).wait_recv()
    for k in range(n - 1):
        for d in both:
            @pl.when(reach(d, k)[1])
            def _(d=d, k=k):
                o_side(1, d, k).wait_recv()
                o_side(2, d, k).wait_recv()

    def rows_of(which):
        rows = pl.ds(pl.multiple_of(which * half, half), half)
        return jnp.concatenate([M[g, k, rows, :] for g in both for k in range(n)], axis=1)

    width = out_ref.shape[1] // n

    def y_copy(j):
        return remote(away.at[j], landed.at[j], y_send.at[j], y_recv.at[j], tp=side)

    def weights_of(j):
        return O[j].reshape(width, 2 * wide)

    theirs = rows_of(side)
    for j in range(n):
        away[j] = nt_dot(theirs, weights_of(j)).astype(jnp.bfloat16)
        if j:
            y_copy(j - 1).start()
    ours = rows_of(x)
    for j in range(n):
        piece = nt_dot(ours, weights_of(j))
        if j == 0:
            y_copy(n - 1).start()
        y_copy(j).wait_recv()
        piece += landed[j].astype(jnp.float32)
        out_ref[:, j * width : (j + 1) * width] = piece.astype(jnp.bfloat16)
    for j in range(n):
        y_copy(j).wait_send()
    for o in range(n):
        for kind in range(3):
            w_side(kind, o).wait_send()
    for o in range(1, n):
        t_copy(o).wait()
        e_copy(o).wait_send()
        w_copy(o).wait_send()
    for kind in range(3):
        o_own(kind).wait_send()
    for k in range(n - 1):
        for d in both:
            @pl.when(reach(d, k)[1])
            def _(d=d, k=k):
                for c in range(PARTS):
                    xx_copy(d, k, c).wait_send()
                for kind in range(3):
                    o_side(kind, d, k).wait_send()

            @pl.when(reach(d, k)[0])
            def _(d=d, k=k):
                for c in range(PARTS):
                    x_copy(d, k, c).wait_send()
                o_copy(d, k).wait_send()


VMEM = pl.BlockSpec(memory_space=pltpu.VMEM)
ANY = pl.BlockSpec(memory_space=pl.ANY)
DMA = pltpu.SemaphoreType.DMA


def on_device_heads(
    n,
    input_layer_rows,
    input_norm_gain,
    query_weight_attention,
    key_weight_attention,
    value_weight_attention,
    query_weight_recurrent,
    forget_weight_recurrent,
    value_weight_recurrent,
    gate_weight_recurrent,
    output_weight_attention,
    emitted_projection_linear_scan,
    score_offset,
    attention_norm_gain,
    recurrence_norm_gain,
    forget_floor,
    forget_offset,
    extra_log_decay,
):
    values = input_layer_rows[0].astype(jnp.float32)
    square_mean = jnp.mean(values * values, axis=-1, keepdims=True)
    normed = (values * lax.rsqrt(square_mean + epsilon) * input_norm_gain).astype(jnp.bfloat16)
    tokens, depth = normed.shape
    groups = lax.axis_size("fs")
    share, columns = query_weight_attention.shape
    width = 7 * HEAD
    half = tokens // 2
    vectors = jnp.stack(
        [jnp.broadcast_to(score_offset[:, None], (n, HEAD))]
        + [
            v.reshape(n, HEAD)
            for v in (attention_norm_gain, recurrence_norm_gain, forget_floor, forget_offset)
        ]
    )
    bf = lambda *shape: pltpu.VMEM(shape, jnp.bfloat16)
    layer_out, T = pl.pallas_call(
        functools.partial(layer_kernel, n),
        out_shape=(
            jax.ShapeDtypeStruct((half, depth), jnp.bfloat16),
            jax.ShapeDtypeStruct((n, 8, tokens), jnp.float32),
        ),
        in_specs=[VMEM] * 3 + [ANY] * 9,
        out_specs=(VMEM,) * 2,
        scratch_shapes=[
            bf(n, tokens, depth),
            bf(n, groups, share, width),
            bf(n, groups, share, 2 * columns),
            bf(n, tokens, HEAD),
            bf(n, share, width),
            bf(n * tokens, width),
            bf(n, tokens, HEAD),
            bf(n, tokens, HEAD),
            pltpu.VMEM((n, 8, tokens), jnp.float32),
            bf(2, n, tokens, HEAD),
            bf(n, half, depth // n),
            bf(n, half, depth // n),
        ]
        + [DMA((2, n, PARTS))] * 4
        + [DMA((2, n))] * 2
        + [DMA((3, n))] * 6
        + [DMA((n,))] * 18
        + [DMA((7, n)), DMA((8,))],
        compiler_params=pltpu.CompilerParams(
            collective_id=0, has_side_effects=True, vmem_limit_bytes=56 * 1024 * 1024
        ),
    )(
        normed,
        extra_log_decay[0].astype(jnp.bfloat16),
        vectors,
        query_weight_attention,
        key_weight_attention,
        value_weight_attention,
        query_weight_recurrent,
        forget_weight_recurrent,
        value_weight_recurrent,
        gate_weight_recurrent,
        output_weight_attention,
        emitted_projection_linear_scan,
    )
    return (layer_out[None], T[:, 0, :][None])


def solution(mesh):
    n = mesh.shape["sp"]
    heads_fit = mesh.shape["fs"] == 4 and mesh.shape["tp"] == 2 and n > 1

    def on_device(*args):
        if heads_fit and args[11].shape[0] == n and args[0].shape[1] == TILE:
            return on_device_heads(n, *args)
        return on_device_general(*args)

    return jax.shard_map(
        on_device,
        mesh=mesh,
        in_specs=(
            P("fs", "sp", None),
            P(),
            P(("sp", "fs"), "tp"),
            P(("sp", "fs"), "tp"),
            P(("sp", "fs"), "tp"),
            P(("sp", "fs"), "tp"),
            P(("sp", "fs"), "tp"),
            P(("sp", "fs"), "tp"),
            P(("sp", "fs"), "tp"),
            P(("sp", "fs"), "tp"),
            P(("sp", "fs"), "tp"),
            P("tp"),
            P("tp"),
            P("tp"),
            P("tp"),
            P("tp"),
            P("fs", "sp", "tp"),
        ),
        out_specs=(P("fs", ("sp", "tp"), None), P("fs", "tp", "sp")),
        check_vma=False,
    )
```

```python
import functools
import jax
import jax.numpy as jnp
from jax import lax
from jax.experimental import pallas as pl
from jax.experimental.pallas import tpu as pltpu
from jax.sharding import PartitionSpec as P

HEAD = 128
BLOCK = 64


epsilon = 1e-06
log_floor = 0.05


def entering(shard, axis, combine, identity):
    size, index = (lax.axis_size(axis), lax.axis_index(axis))
    everything = jax.tree.map(
        lambda part, kind: lax.all_gather(part.astype(kind), axis),
        shard,
        (jnp.bfloat16, jnp.bfloat16),
    )
    start = jax.tree.map(
        lambda part, zero: jnp.broadcast_to(jnp.asarray(zero, part.dtype), part.shape),
        shard,
        identity,
    )

    def hop(k, before):
        reached = k < index
        new = combine(
            before, jax.tree.map(lambda part, own: part[k].astype(own.dtype), everything, shard)
        )
        return jax.tree.map(lambda a, b: jnp.where(reached, a, b), new, before)

    return lax.fori_loop(0, size, hop, start)


def head_norm(values, gain):
    square_mean = jnp.mean(values * values, axis=-1, keepdims=True)
    return values * lax.rsqrt(square_mean + epsilon) * gain


def recurrence_block(memory_matrix, inputs):
    query_slice, decay_part, key_slice, value_slice = inputs
    highest_score = lax.Precision.HIGHEST
    length = decay_part.shape[0]
    running_total = jnp.cumsum(decay_part, axis=0)
    causal = (
        lax.broadcasted_iota(jnp.int32, (length, length), 0)
        >= lax.broadcasted_iota(jnp.int32, (length, length), 1)
    )[:, :, None, None]
    relative = jnp.where(causal, running_total[:, None] - running_total[None, :], -jnp.inf)
    pairwise = jnp.sum(query_slice[:, None] * key_slice[None, :] * jnp.exp(relative), axis=-1)
    inner_part = jnp.einsum("tsh,shv->thv", pairwise, value_slice, precision=highest_score)
    carried_state = jnp.einsum(
        "fby,bym->fbm", query_slice * jnp.exp(running_total), memory_matrix, precision=highest_score
    )
    final_total = running_total[-1]
    updated_state = jnp.exp(final_total)[:, :, None] * memory_matrix + jnp.einsum(
        "rxc,rxa->xca",
        key_slice * jnp.exp(final_total[None] - running_total),
        value_slice,
        precision=highest_score,
    )
    return (updated_state, inner_part + carried_state)


def stick_piece(queries, shifts, weighted, keep_total, key_value, is_own, is_valid):
    scores = (
        jnp.einsum("thd,shd->hts", queries, key_value[0], preferred_element_type=jnp.float32)
        * HEAD ** (-0.5)
        + shifts[:, None, None]
    )
    logarithmic_retention = jax.nn.log_sigmoid(-scores)
    if is_own:
        rows_here = scores.shape[1]
        strict = lax.broadcasted_iota(jnp.int32, (rows_here, rows_here), 0) > lax.broadcasted_iota(
            jnp.int32, (rows_here, rows_here), 1
        )
        logarithmic_retention = jnp.where(strict, logarithmic_retention, 0.0)
    suffix = lax.cumsum(logarithmic_retention, axis=2, reverse=True) - logarithmic_retention
    log_weight = jax.nn.log_sigmoid(scores) + suffix + keep_total[:, :, None]
    if is_own:
        log_weight = jnp.where(strict, log_weight, -jnp.inf)
    weights = jnp.where(is_valid, jnp.exp(log_weight), 0.0).astype(jnp.bfloat16)
    weighted = weighted + jnp.einsum(
        "hts,shd->thd", weights, key_value[1], preferred_element_type=jnp.float32
    )
    keep_total = keep_total + jnp.where(is_valid, jnp.sum(logarithmic_retention, axis=2), 0.0)
    return (weighted, keep_total)


def contract_rows(rows_in, weight):
    return lax.dot_general(
        rows_in, weight, (((1,), (1,)), ((), ())), preferred_element_type=jnp.float32
    )


def on_device_general(
    input_layer_rows,
    input_norm_gain,
    query_weight_attention,
    key_weight_attention,
    value_weight_attention,
    query_weight_recurrent,
    forget_weight_recurrent,
    value_weight_recurrent,
    gate_weight_recurrent,
    output_weight_attention,
    emitted_projection_linear_scan,
    score_offset,
    attention_norm_gain,
    recurrence_norm_gain,
    forget_floor,
    forget_offset,
    extra_log_decay,
):
    values = input_layer_rows[0].astype(jnp.float32)
    square_mean = jnp.mean(values * values, axis=-1, keepdims=True)
    normed = (values * lax.rsqrt(square_mean + epsilon) * input_norm_gain).astype(jnp.bfloat16)
    tokens = normed.shape[0]
    weights_in = (
        query_weight_attention,
        key_weight_attention,
        value_weight_attention,
        query_weight_recurrent,
        forget_weight_recurrent,
        value_weight_recurrent,
        gate_weight_recurrent,
    )
    pieces = (
        lax.all_gather(weights_in[0], ("sp", "fs"), axis=0, tiled=True),
        lax.all_gather(weights_in[1], ("sp", "fs"), axis=0, tiled=True),
        lax.all_gather(weights_in[2], ("sp", "fs"), axis=0, tiled=True),
        lax.all_gather(weights_in[3], ("sp", "fs"), axis=0, tiled=True),
        lax.all_gather(weights_in[4], ("sp", "fs"), axis=0, tiled=True),
        lax.all_gather(weights_in[5], ("sp", "fs"), axis=0, tiled=True),
        lax.all_gather(weights_in[6], ("sp", "fs"), axis=0, tiled=True),
    )
    projected = tuple(
        (jnp.dot(normed, weight, preferred_element_type=jnp.float32) for weight in pieces)
    )
    query_a, key_a, value_a, query_b, forget_b, input_b, gate_b = [
        column_block.astype(jnp.bfloat16) for column_block in projected
    ]
    out_a, out_b = (
        lax.all_gather(output_weight_attention, ("sp", "fs"), axis=0, tiled=True),
        lax.all_gather(emitted_projection_linear_scan, ("sp", "fs"), axis=0, tiled=True),
    )
    head_count = query_a.shape[1] // HEAD
    queries = query_a.reshape(tokens, head_count, HEAD)
    key_value = jnp.stack(
        [key_a.reshape(tokens, head_count, HEAD), value_a.reshape(tokens, head_count, HEAD)]
    )
    weighted = jnp.zeros((tokens, head_count, HEAD), jnp.float32)
    keep_total = jnp.zeros((head_count, tokens), jnp.float32)
    weighted, keep_total = stick_piece(
        queries, score_offset, weighted, keep_total, key_value, True, True
    )
    position = lax.axis_index("sp")
    seq_devices = lax.axis_size("sp")
    gathered = lax.all_gather(key_value, "sp", axis=1, tiled=True)

    def gathered_turn(turn_index, carried_state):
        weighted_now, keep_now = carried_state
        source = jnp.maximum(position - turn_index, 0) * tokens
        piece_pair = lax.dynamic_slice_in_dim(gathered, source, tokens, 1)
        return stick_piece(
            queries, score_offset, weighted_now, keep_now, piece_pair, False, position >= turn_index
        )

    weighted, keep_total = lax.fori_loop(1, seq_devices, gathered_turn, (weighted, keep_total))
    row_log_total = jnp.log(jnp.maximum(-jnp.expm1(keep_total), log_floor))[None]
    mixed_a = (
        head_norm(weighted, attention_norm_gain.reshape(head_count, HEAD))
        .reshape(tokens, head_count * HEAD)
        .astype(jnp.bfloat16)
    )
    forget_logits = forget_b.astype(jnp.float32) + forget_offset
    forget_log_value = (
        jnp.logaddexp(
            jnp.log(forget_floor), jnp.log1p(-forget_floor) + jax.nn.log_sigmoid(forget_logits)
        )
        + extra_log_decay[0]
    )
    key_in = (1.0 - forget_floor) * jax.nn.sigmoid(-forget_logits)
    query_rows_input = jax.nn.silu(query_b.astype(jnp.float32)).reshape(tokens, head_count, HEAD)
    value_in = input_b.astype(jnp.float32)
    fading_channel_groups = forget_log_value.reshape(tokens, head_count, HEAD)
    shaped = tuple(
        (
            array_in.reshape(tokens // BLOCK, BLOCK, head_count, HEAD)
            for array_in in (query_rows_input, forget_log_value, key_in, value_in)
        )
    )
    empty_state = jnp.zeros((head_count, HEAD, HEAD), jnp.float32)
    nearby_hidden_vector, local_out = lax.scan(recurrence_block, empty_state, shaped)
    local_out = local_out.reshape(tokens, head_count, HEAD)
    through = jnp.exp(jnp.sum(fading_channel_groups, axis=0))

    def chain_states(earlier, later):
        return (earlier[0] * later[0], later[0][:, :, None] * earlier[1] + later[1])

    identity = (jnp.ones_like(through), jnp.zeros_like(nearby_hidden_vector))
    unused_decay, incoming_state = entering(
        (through, nearby_hidden_vector), "sp", chain_states, identity
    )
    running_sum = jnp.cumsum(fading_channel_groups, axis=0)
    recurrent = local_out + jnp.einsum(
        "fby,bym->fbm",
        query_rows_input * jnp.exp(running_sum),
        incoming_state,
        precision=lax.Precision.HIGHEST,
    )
    gated_out = head_norm(recurrent, recurrence_norm_gain.reshape(head_count, HEAD)) * jax.nn.silu(
        gate_b.astype(jnp.float32).reshape(tokens, head_count, HEAD)
    )
    mixed_b = gated_out.reshape(tokens, head_count * HEAD).astype(jnp.bfloat16)
    summed = lax.psum_scatter(
        (contract_rows(mixed_a, out_a) + contract_rows(mixed_b, out_b)).astype(jnp.bfloat16),
        "tp",
        scatter_dimension=0,
        tiled=True,
    )
    layer_out = summed[None]
    return (layer_out, row_log_total)


LEAF = 16
CHUNK = 128
TILE = 256
MESH = pl.DeviceIdType.MESH


def remote(src, dst, send, recv, **where):
    return pltpu.make_async_remote_copy(
        src_ref=src, dst_ref=dst, send_sem=send, recv_sem=recv, device_id=where, device_id_type=MESH
    )


def greet(peers):
    barrier = pltpu.get_barrier_semaphore()
    for where in peers:
        pl.semaphore_signal(barrier, inc=1, device_id=where, device_id_type=MESH)
    pl.semaphore_wait(barrier, len(peers))


def nt_dot(a, b):
    return lax.dot_general(a, b, (((1,), (1,)), ((), ())), preferred_element_type=jnp.float32)


def tn_dot(a, b):
    return lax.dot_general(a, b, (((0,), (0,)), ((), ())), preferred_element_type=jnp.float32)


def grid_of(shape):
    return lax.broadcasted_iota(jnp.int32, shape, 0), lax.broadcasted_iota(jnp.int32, shape, 1)


def attend_tile(i, p_ref, shift, gain):
    here = slice(i * TILE, (i + 1) * TILE)
    r, c = grid_of((TILE, TILE))
    later = (r > c).astype(jnp.bfloat16)
    query = p_ref[here, 0:HEAD]
    total = jnp.zeros((TILE, HEAD), jnp.float32)
    keep = jnp.zeros((TILE, 1), jnp.float32)
    for j in range(i, -1, -1):
        there = slice(j * TILE, (j + 1) * TILE)
        score = nt_dot(query, p_ref[there, HEAD : 2 * HEAD]) * HEAD ** (-0.5) + shift
        soft = -(jnp.maximum(score, 0.0) + jnp.log1p(jnp.exp(-jnp.abs(score))))
        held = jnp.where(r > c, soft, 0.0) if i == j else soft
        high = held.astype(jnp.bfloat16)
        low = (held - high.astype(jnp.float32)).astype(jnp.bfloat16)
        suffix = jnp.dot(high, later, preferred_element_type=jnp.float32) + jnp.dot(
            low, later, preferred_element_type=jnp.float32
        )
        weight = jnp.exp(score + soft + suffix + keep)
        if i == j:
            weight = jnp.where(r > c, weight, 0.0)
        total += jnp.dot(
            weight.astype(jnp.bfloat16),
            p_ref[there, 2 * HEAD : 3 * HEAD],
            preferred_element_type=jnp.float32,
        )
        keep += jnp.sum(held, axis=1, keepdims=True)
    return head_norm(total, gain).astype(jnp.bfloat16), keep


def recur_chunk(p_ref, e_ref, here, state, floor, offset, gain):
    r, c = grid_of((CHUNK, CHUNK))
    lower = (r >= c).astype(jnp.float32)
    part = lambda k: p_ref[here, k * HEAD : (k + 1) * HEAD].astype(jnp.float32)
    raw = part(3)
    query = raw * jax.nn.sigmoid(raw)
    key = (1.0 - floor) * jax.nn.sigmoid(-(part(4) + offset))
    value = p_ref[here, 5 * HEAD : 6 * HEAD]
    gate = part(6)
    decay = jnp.log1p(-key) + e_ref[...].astype(jnp.float32)
    run = jnp.dot(lower, decay, precision=lax.Precision.HIGHEST, preferred_element_type=jnp.float32)
    stripes = [jnp.zeros((LEAF, CHUNK), jnp.float32)]
    for s in range(LEAF, CHUNK, LEAF):
        edge = run[s - 1 : s, :]
        near = (query[s : s + LEAF] * jnp.exp(run[s : s + LEAF] - edge)).astype(jnp.bfloat16)
        far = (key * jnp.exp(jnp.where(r < s, edge - run, -jnp.inf))).astype(jnp.bfloat16)
        stripes.append(nt_dot(near, far))
    pairs = jnp.concatenate(stripes, axis=0)
    for d in range(LEAF):
        back_key = pltpu.roll(key, d, 0) if d else key
        back_run = pltpu.roll(run, d, 0) if d else run
        gap = jnp.where(r % LEAF >= d, run - back_run, -jnp.inf)
        column = jnp.sum(query * back_key * jnp.exp(gap), axis=1, keepdims=True)
        pairs = jnp.where((r - c == d) & (r % LEAF >= d), column, pairs)
    last = run[CHUNK - 1 : CHUNK, :]
    out = jnp.dot(pairs.astype(jnp.bfloat16), value, preferred_element_type=jnp.float32)
    out += nt_dot((query * jnp.exp(run)).astype(jnp.bfloat16), state.astype(jnp.bfloat16))
    mixed = head_norm(out, gain) * (gate * jax.nn.sigmoid(gate))
    state = jnp.exp(last) * state + tn_dot(value, (key * jnp.exp(last - run)).astype(jnp.bfloat16))
    return mixed.astype(jnp.bfloat16), state


PARTS = 4


def layer_kernel(n, *refs):
    raw_ref, g_ref, xe_ref, v_ref = refs[:4]
    w_refs, o_refs = refs[4:11], refs[11:13]
    out_ref, T = refs[13:15]
    (
        X, W, O, E, x_ref, e_ref, wp, proj, ma, mb, ts, M, away, landed,
        x_send, x_recv, xx_send, xx_recv,
        o_send, o_recv, oy_send, oy_recv, oc_send, oc_recv, od_send, od_recv,
        w_send, w_recv, wy_send, wy_recv, wc_send, wc_recv, wd_send, wd_recv,
        e_send, e_recv, m_send, m_recv, b_send, b_recv, t_send, t_recv, y_send, y_recv,
        pack_sem, local_sem,
    ) = refs[15:]
    z, f, x = lax.axis_index("sp"), lax.axis_index("fs"), lax.axis_index("tp")
    core, row, side = f + 1 - 2 * (f % 2), (f + 2) % 4, 1 - x
    tokens = x_ref.shape[0]
    half = tokens // 2
    step = half // PARTS
    both = (0, 1)

    def cols(h):
        return pl.ds(pl.multiple_of(h * HEAD, HEAD), HEAD)

    packs = []
    for i, w in enumerate(w_refs):
        for h in range(n):
            packs.append(
                pltpu.make_async_copy(
                    w.at[:, h * HEAD : (h + 1) * HEAD],
                    wp.at[h, :, i * HEAD : (i + 1) * HEAD],
                    pack_sem.at[i, h],
                )
            )
    wide = o_refs[0].shape[1]
    for i, o in enumerate(o_refs):
        packs.append(
            pltpu.make_async_copy(o, O.at[z, f, :, i * wide : (i + 1) * wide], local_sem.at[i])
        )
    for copy in packs:
        copy.start()
    barrier = pltpu.get_barrier_semaphore()
    peers = [{"sp": (z + o) % n} for o in range(1, n)] + [{"fs": core}, {"fs": row}, {"tp": side}]
    for where in peers:
        pl.semaphore_signal(barrier, inc=1, device_id=where, device_id_type=MESH)

    def normalise(i, carry):
        rows = pl.ds(pl.multiple_of(i * step, step), step)
        x_ref[rows, :] = head_norm(raw_ref[rows, :].astype(jnp.float32), g_ref[...]).astype(jnp.bfloat16)
        return carry

    lax.fori_loop(0, tokens // step, normalise, 0)
    for copy in packs:
        copy.wait()
    pl.semaphore_wait(barrier, len(peers))
    own_w = pltpu.make_async_copy(wp.at[z], W.at[z, f], local_sem.at[4])
    own_w.start()

    def reach(direction, k):
        if direction == 0:
            return (z - k >= 0) & (z + 1 < n), z - 1 - k >= 0, z - k, z - 1 - k, z + 1
        return (z + k < n) & (z - 1 >= 0), z + 1 + k < n, z + k, z + 1 + k, z - 1

    def span(c):
        return pl.ds(pl.multiple_of(x * half + c * step, step), step)

    def x_copy(direction, k, c, first=False):
        _, _, out, _, to = reach(direction, k)
        src = x_ref.at[span(c)] if first else X.at[out, span(c)]
        return remote(
            src, X.at[out, span(c)], x_send.at[direction, k, c], x_recv.at[direction, k, c], sp=to
        )

    def x_wait(direction, k, c):
        block = X.at[reach(direction, k)[3], span(c)]
        return remote(block, block, x_send.at[direction, k, c], x_recv.at[direction, k, c], sp=(z + 1) % n)

    def xx_copy(direction, k, c):
        block = X.at[reach(direction, k)[3], span(c)]
        return remote(block, block, xx_send.at[direction, k, c], xx_recv.at[direction, k, c], tp=side)

    def xx_wait(direction, k, c):
        there = pl.ds(pl.multiple_of(side * half + c * step, step), step)
        block = X.at[reach(direction, k)[3], there]
        return remote(block, block, xx_send.at[direction, k, c], xx_recv.at[direction, k, c], tp=side)

    def o_copy(direction, k):
        _, _, out, _, to = reach(direction, k)
        return remote(O.at[out, f], O.at[out, f], o_send.at[direction, k], o_recv.at[direction, k], sp=to)

    def o_side(kind, direction, k, own=False):
        block = z if own else reach(direction, k)[3]
        send, recv = ((oy_send, oy_recv), (oc_send, oc_recv), (od_send, od_recv))[kind]
        piece = O.at[block, row if kind == 2 else f]
        where = {"fs": row if kind == 0 else core}
        return remote(piece, piece, send.at[direction, k], recv.at[direction, k], **where)

    def o_own(kind):
        return o_side(kind, 2, 0, own=True)

    def w_copy(o):
        return remote(wp.at[(z + o) % n], W.at[z, f], w_send.at[o], w_recv.at[o], sp=(z + o) % n)

    def e_copy(o):
        return remote(e_ref.at[:, cols((z + o) % n)], E.at[z], e_send.at[o], e_recv.at[o], sp=(z + o) % n)

    def w_side(kind, o):
        block = (z - o + n) % n
        src = wp.at[z] if o == 0 else W.at[block, f]
        if kind == 0:
            return remote(src, W.at[block, f], wy_send.at[o], wy_recv.at[o], fs=row)
        if kind == 1:
            return remote(src, W.at[block, f], wc_send.at[o], wc_recv.at[o], fs=core)
        return remote(W.at[block, row], W.at[block, row], wd_send.at[o], wd_recv.at[o], fs=core)

    for d in both:
        @pl.when(reach(d, 0)[0])
        def _(d=d):
            for c in range(PARTS):
                x_copy(d, 0, c, True).start()
    for o in range(1, n):
        w_copy(o).start()
    for kind in both:
        w_side(kind, 0).start()
    local = [
        pltpu.make_async_copy(x_ref, X.at[z], local_sem.at[2]),
        pltpu.make_async_copy(e_ref.at[:, cols(z)], E.at[z], local_sem.at[3]),
    ]
    local[0].start()
    e_ref[...] = xe_ref[...].astype(jnp.bfloat16)

    def o_begin(direction, when):
        @pl.when(when & reach(direction, 0)[0])
        def _():
            o_copy(direction, 0).start()

    o_begin(0, z == 0)
    o_begin(1, z == n - 1)
    local[0].wait()
    own_w.wait()

    def project(block):
        rows = X[block]
        weights = W[...].reshape(rows.shape[1], W.shape[3])
        made = jnp.dot(rows, weights, preferred_element_type=jnp.float32)
        at = pl.ds(pl.multiple_of(block * tokens, tokens), tokens)
        proj[at, :] = made.astype(jnp.bfloat16)

    def gather_step(k, carry):
        for d in both:
            @pl.when((k < n - 1) & reach(d, k)[1])
            def _(d=d):
                for c in range(PARTS):
                    x_wait(d, k, c).wait_recv()

                    @pl.when(reach(d, k + 1)[0])
                    def _(c=c):
                        x_copy(d, k + 1, c).start()
                    xx_copy(d, k, c).start()

        @pl.when(k == max(n - 3, 0))
        def _():
            local[1].start()
            for o in range(1, n):
                e_copy(o).start()

        o_begin(0, (z > 0) & (k == z - 1))
        o_begin(1, (z < n - 1) & (k == n - 2 - z))

        @pl.when(k == 0)
        def _():
            for o in range(1, n):
                w_copy(o).wait_recv()
                for kind in both:
                    w_side(kind, o).start()
            for kind in both:
                o_own(kind).start()
            for o in range(n):
                w_side(0, o).wait_recv()
                w_side(2, o).start()
            for o in range(n):
                w_side(1, o).wait_recv()
                w_side(2, o).wait_recv()

        @pl.when(z - k >= 0)
        def _():
            @pl.when(k > 0)
            def _():
                for c in range(PARTS):
                    xx_wait(0, k - 1, c).wait_recv()
            project(z - k)

        @pl.when((k > 0) & (z + k < n))
        def _():
            for c in range(PARTS):
                xx_wait(1, k - 1, c).wait_recv()
            project(z + k)
        return carry

    lax.fori_loop(0, n, gather_step, 0)

    def o_tick(k):
        for d in both:
            @pl.when(reach(d, k)[1])
            def _(d=d):
                o_copy_in = O.at[reach(d, k)[3], f]
                remote(o_copy_in, o_copy_in, o_send.at[d, k], o_recv.at[d, k], sp=(z + 1) % n).wait_recv()
                if k + 1 < n - 1:
                    @pl.when(reach(d, k + 1)[0])
                    def _():
                        o_copy(d, k + 1).start()
                for kind in both:
                    o_side(kind, d, k).start()

    def m_copy(o):
        return remote(ma.at[(z + o) % n], M.at[0, z], m_send.at[o], m_recv.at[o], sp=(z + o) % n)

    def b_copy(o):
        return remote(mb.at[(z + o) % n], M.at[1, z], b_send.at[o], b_recv.at[o], sp=(z + o) % n)

    def t_copy(o):
        return remote(ts.at[(z + o) % n], T.at[z], t_send.at[o], t_recv.at[o], sp=(z + o) % n)

    o_tick(0)
    param = lambda i: v_ref[i, pl.ds(z, 1), :]
    shift = param(0)[:, 0:1]
    for i in range(n):
        mixed, keep = attend_tile(i, proj, shift, param(1))
        ma[i] = mixed
        total = jnp.log(jnp.maximum(1.0 - jnp.exp(keep), log_floor))
        ts[i] = jnp.broadcast_to(total, (tokens, HEAD)).T[0:8, :]
    local[1].wait()
    for o in range(1, n):
        e_copy(o).wait_recv()
    floor, offset, gain = param(3), param(4), param(2)
    per = tokens // CHUNK

    def chunk(i, state):
        here = pl.ds(pl.multiple_of(i * CHUNK, CHUNK), CHUNK)
        at = pl.ds(pl.multiple_of((i % per) * CHUNK, CHUNK), CHUNK)
        extra = E.at[i // per, at]
        mixed, state = recur_chunk(proj, extra, here, state, floor, offset, gain)
        mb[i // per, at, :] = mixed
        return state

    state = jnp.zeros((HEAD, HEAD), jnp.float32)
    count = per * n
    state = lax.fori_loop(0, count // 4, chunk, state)
    for o in range(1, n):
        m_copy(o).start()
    for o in range(1, n):
        t_copy(o).start()
    if n > 2:
        o_tick(1)
    lax.fori_loop(count // 4, count, chunk, state)
    mine = [
        pltpu.make_async_copy(ma.at[z], M.at[0, z], local_sem.at[5]),
        pltpu.make_async_copy(mb.at[z], M.at[1, z], local_sem.at[6]),
        pltpu.make_async_copy(ts.at[z], T.at[z], local_sem.at[7]),
    ]
    for copy in mine:
        copy.start()
    for o in range(1, n):
        b_copy(o).start()
    o_own(0).wait_recv()
    o_own(2).start()
    for k in range(2, n - 1):
        o_tick(k)
    o_own(1).wait_recv()
    o_own(2).wait_recv()
    for copy in mine:
        copy.wait()
    for o in range(1, n):
        m_copy(o).wait()
        b_copy(o).wait()

    shorter = jnp.minimum(z, n - 1 - z)

    def hop_of(s):
        t = s - 1
        paired = t < 2 * shorter
        k = jnp.where(paired, t // 2, t - shorter)
        d = jnp.where(paired, t % 2, jnp.where(z > n - 1 - z, 0, 1))
        return d, k, jnp.where(d == 0, z - 1 - k, z + 1 + k)

    def o_late(kind, s):
        d, k, block = hop_of(s)
        send, recv = ((oy_send, oy_recv), (oc_send, oc_recv), (od_send, od_recv))[kind]
        piece = O.at[block, row if kind == 2 else f]
        where = {"fs": row if kind == 0 else core}
        return remote(piece, piece, send.at[d, k], recv.at[d, k], **where)

    def rows_of(which):
        rows = pl.ds(pl.multiple_of(which * half, half), half)
        return jnp.concatenate([M[g, k, rows, :] for g in both for k in range(n)], axis=1)

    width = out_ref.shape[1] // n

    def y_copy(j):
        return remote(away.at[j], landed.at[j], y_send.at[j], y_recv.at[j], tp=side)

    def weights_of(block):
        return O[block].reshape(width, 2 * wide)

    theirs = rows_of(side)
    o_late(0, 1).wait_recv()
    o_late(2, 1).start()
    for j in range(n):
        if j:
            o_late(1, j).wait_recv()
            o_late(2, j).wait_recv()
        away[j] = nt_dot(theirs, weights_of(hop_of(j)[2] if j else z)).astype(jnp.bfloat16)
        if j:
            y_copy(j - 1).start()
            if j + 1 < n:
                o_late(0, j + 1).wait_recv()
                o_late(2, j + 1).start()
    ours = rows_of(x)
    for j in range(n):
        block = hop_of(j)[2] if j else z
        piece = nt_dot(ours, weights_of(block))
        if j == 0:
            y_copy(n - 1).start()
        y_copy(j).wait_recv()
        piece += landed[j].astype(jnp.float32)
        out_ref[:, pl.ds(pl.multiple_of(block * width, width), width)] = piece.astype(jnp.bfloat16)
    for j in range(n):
        y_copy(j).wait_send()
    for o in range(n):
        for kind in range(3):
            w_side(kind, o).wait_send()
    for o in range(1, n):
        t_copy(o).wait()
        e_copy(o).wait_send()
        w_copy(o).wait_send()
    for kind in range(3):
        o_own(kind).wait_send()
    for k in range(n - 1):
        for d in both:
            @pl.when(reach(d, k)[1])
            def _(d=d, k=k):
                for c in range(PARTS):
                    xx_copy(d, k, c).wait_send()
                for kind in range(3):
                    o_side(kind, d, k).wait_send()

            @pl.when(reach(d, k)[0])
            def _(d=d, k=k):
                for c in range(PARTS):
                    x_copy(d, k, c).wait_send()
                o_copy(d, k).wait_send()


VMEM = pl.BlockSpec(memory_space=pltpu.VMEM)
ANY = pl.BlockSpec(memory_space=pl.ANY)
DMA = pltpu.SemaphoreType.DMA


def on_device_heads(
    n,
    input_layer_rows,
    input_norm_gain,
    query_weight_attention,
    key_weight_attention,
    value_weight_attention,
    query_weight_recurrent,
    forget_weight_recurrent,
    value_weight_recurrent,
    gate_weight_recurrent,
    output_weight_attention,
    emitted_projection_linear_scan,
    score_offset,
    attention_norm_gain,
    recurrence_norm_gain,
    forget_floor,
    forget_offset,
    extra_log_decay,
):
    _, tokens, depth = input_layer_rows.shape
    groups = lax.axis_size("fs")
    share, columns = query_weight_attention.shape
    width = 7 * HEAD
    half = tokens // 2
    vectors = jnp.stack(
        [jnp.broadcast_to(score_offset[:, None], (n, HEAD))]
        + [
            v.reshape(n, HEAD)
            for v in (attention_norm_gain, recurrence_norm_gain, forget_floor, forget_offset)
        ]
    )
    bf = lambda *shape: pltpu.VMEM(shape, jnp.bfloat16)
    layer_out, T = pl.pallas_call(
        functools.partial(layer_kernel, n),
        out_shape=(
            jax.ShapeDtypeStruct((half, depth), jnp.bfloat16),
            jax.ShapeDtypeStruct((n, 8, tokens), jnp.float32),
        ),
        in_specs=[VMEM] * 4 + [ANY] * 9,
        out_specs=(VMEM,) * 2,
        scratch_shapes=[
            bf(n, tokens, depth),
            bf(n, groups, share, width),
            bf(n, groups, share, 2 * columns),
            bf(n, tokens, HEAD),
            bf(tokens, depth),
            bf(tokens, columns),
            bf(n, share, width),
            bf(n * tokens, width),
            bf(n, tokens, HEAD),
            bf(n, tokens, HEAD),
            pltpu.VMEM((n, 8, tokens), jnp.float32),
            bf(2, n, tokens, HEAD),
            bf(n, half, depth // n),
            bf(n, half, depth // n),
        ]
        + [DMA((2, n, PARTS))] * 4
        + [DMA((2, n))] * 2
        + [DMA((3, n))] * 6
        + [DMA((n,))] * 18
        + [DMA((7, n)), DMA((8,))],
        compiler_params=pltpu.CompilerParams(
            collective_id=0, has_side_effects=True, vmem_limit_bytes=56 * 1024 * 1024
        ),
    )(
        input_layer_rows[0],
        input_norm_gain[None],
        extra_log_decay[0],
        vectors,
        query_weight_attention,
        key_weight_attention,
        value_weight_attention,
        query_weight_recurrent,
        forget_weight_recurrent,
        value_weight_recurrent,
        gate_weight_recurrent,
        output_weight_attention,
        emitted_projection_linear_scan,
    )
    return (layer_out[None], T[:, 0, :][None])


def solution(mesh):
    n = mesh.shape["sp"]
    heads_fit = mesh.shape["fs"] == 4 and mesh.shape["tp"] == 2 and n > 1

    def on_device(*args):
        if heads_fit and args[11].shape[0] == n and args[0].shape[1] == TILE:
            return on_device_heads(n, *args)
        return on_device_general(*args)

    return jax.shard_map(
        on_device,
        mesh=mesh,
        in_specs=(
            P("fs", "sp", None),
            P(),
            P(("sp", "fs"), "tp"),
            P(("sp", "fs"), "tp"),
            P(("sp", "fs"), "tp"),
            P(("sp", "fs"), "tp"),
            P(("sp", "fs"), "tp"),
            P(("sp", "fs"), "tp"),
            P(("sp", "fs"), "tp"),
            P(("sp", "fs"), "tp"),
            P(("sp", "fs"), "tp"),
            P("tp"),
            P("tp"),
            P("tp"),
            P("tp"),
            P("tp"),
            P("fs", "sp", "tp"),
        ),
        out_specs=(P("fs", ("sp", "tp"), None), P("fs", "tp", "sp")),
        check_vma=False,
    )
```

```python
import functools
import jax
import jax.numpy as jnp
from jax import lax
from jax.experimental import pallas as pl
from jax.experimental.pallas import tpu as pltpu
from jax.sharding import PartitionSpec as P

HEAD = 128
BLOCK = 64


epsilon = 1e-06
log_floor = 0.05


def entering(shard, axis, combine, identity):
    size, index = (lax.axis_size(axis), lax.axis_index(axis))
    everything = jax.tree.map(
        lambda part, kind: lax.all_gather(part.astype(kind), axis),
        shard,
        (jnp.bfloat16, jnp.bfloat16),
    )
    start = jax.tree.map(
        lambda part, zero: jnp.broadcast_to(jnp.asarray(zero, part.dtype), part.shape),
        shard,
        identity,
    )

    def hop(k, before):
        reached = k < index
        new = combine(
            before, jax.tree.map(lambda part, own: part[k].astype(own.dtype), everything, shard)
        )
        return jax.tree.map(lambda a, b: jnp.where(reached, a, b), new, before)

    return lax.fori_loop(0, size, hop, start)


def head_norm(values, gain):
    square_mean = jnp.mean(values * values, axis=-1, keepdims=True)
    return values * lax.rsqrt(square_mean + epsilon) * gain


def recurrence_block(memory_matrix, inputs):
    query_slice, decay_part, key_slice, value_slice = inputs
    highest_score = lax.Precision.HIGHEST
    length = decay_part.shape[0]
    running_total = jnp.cumsum(decay_part, axis=0)
    causal = (
        lax.broadcasted_iota(jnp.int32, (length, length), 0)
        >= lax.broadcasted_iota(jnp.int32, (length, length), 1)
    )[:, :, None, None]
    relative = jnp.where(causal, running_total[:, None] - running_total[None, :], -jnp.inf)
    pairwise = jnp.sum(query_slice[:, None] * key_slice[None, :] * jnp.exp(relative), axis=-1)
    inner_part = jnp.einsum("tsh,shv->thv", pairwise, value_slice, precision=highest_score)
    carried_state = jnp.einsum(
        "fby,bym->fbm", query_slice * jnp.exp(running_total), memory_matrix, precision=highest_score
    )
    final_total = running_total[-1]
    updated_state = jnp.exp(final_total)[:, :, None] * memory_matrix + jnp.einsum(
        "rxc,rxa->xca",
        key_slice * jnp.exp(final_total[None] - running_total),
        value_slice,
        precision=highest_score,
    )
    return (updated_state, inner_part + carried_state)


def stick_piece(queries, shifts, weighted, keep_total, key_value, is_own, is_valid):
    scores = (
        jnp.einsum("thd,shd->hts", queries, key_value[0], preferred_element_type=jnp.float32)
        * HEAD ** (-0.5)
        + shifts[:, None, None]
    )
    logarithmic_retention = jax.nn.log_sigmoid(-scores)
    if is_own:
        rows_here = scores.shape[1]
        strict = lax.broadcasted_iota(jnp.int32, (rows_here, rows_here), 0) > lax.broadcasted_iota(
            jnp.int32, (rows_here, rows_here), 1
        )
        logarithmic_retention = jnp.where(strict, logarithmic_retention, 0.0)
    suffix = lax.cumsum(logarithmic_retention, axis=2, reverse=True) - logarithmic_retention
    log_weight = jax.nn.log_sigmoid(scores) + suffix + keep_total[:, :, None]
    if is_own:
        log_weight = jnp.where(strict, log_weight, -jnp.inf)
    weights = jnp.where(is_valid, jnp.exp(log_weight), 0.0).astype(jnp.bfloat16)
    weighted = weighted + jnp.einsum(
        "hts,shd->thd", weights, key_value[1], preferred_element_type=jnp.float32
    )
    keep_total = keep_total + jnp.where(is_valid, jnp.sum(logarithmic_retention, axis=2), 0.0)
    return (weighted, keep_total)


def contract_rows(rows_in, weight):
    return lax.dot_general(
        rows_in, weight, (((1,), (1,)), ((), ())), preferred_element_type=jnp.float32
    )


def on_device_general(
    input_layer_rows,
    input_norm_gain,
    query_weight_attention,
    key_weight_attention,
    value_weight_attention,
    query_weight_recurrent,
    forget_weight_recurrent,
    value_weight_recurrent,
    gate_weight_recurrent,
    output_weight_attention,
    emitted_projection_linear_scan,
    score_offset,
    attention_norm_gain,
    recurrence_norm_gain,
    forget_floor,
    forget_offset,
    extra_log_decay,
):
    values = input_layer_rows[0].astype(jnp.float32)
    square_mean = jnp.mean(values * values, axis=-1, keepdims=True)
    normed = (values * lax.rsqrt(square_mean + epsilon) * input_norm_gain).astype(jnp.bfloat16)
    tokens = normed.shape[0]
    weights_in = (
        query_weight_attention,
        key_weight_attention,
        value_weight_attention,
        query_weight_recurrent,
        forget_weight_recurrent,
        value_weight_recurrent,
        gate_weight_recurrent,
    )
    pieces = (
        lax.all_gather(weights_in[0], ("sp", "fs"), axis=0, tiled=True),
        lax.all_gather(weights_in[1], ("sp", "fs"), axis=0, tiled=True),
        lax.all_gather(weights_in[2], ("sp", "fs"), axis=0, tiled=True),
        lax.all_gather(weights_in[3], ("sp", "fs"), axis=0, tiled=True),
        lax.all_gather(weights_in[4], ("sp", "fs"), axis=0, tiled=True),
        lax.all_gather(weights_in[5], ("sp", "fs"), axis=0, tiled=True),
        lax.all_gather(weights_in[6], ("sp", "fs"), axis=0, tiled=True),
    )
    projected = tuple(
        (jnp.dot(normed, weight, preferred_element_type=jnp.float32) for weight in pieces)
    )
    query_a, key_a, value_a, query_b, forget_b, input_b, gate_b = [
        column_block.astype(jnp.bfloat16) for column_block in projected
    ]
    out_a, out_b = (
        lax.all_gather(output_weight_attention, ("sp", "fs"), axis=0, tiled=True),
        lax.all_gather(emitted_projection_linear_scan, ("sp", "fs"), axis=0, tiled=True),
    )
    head_count = query_a.shape[1] // HEAD
    queries = query_a.reshape(tokens, head_count, HEAD)
    key_value = jnp.stack(
        [key_a.reshape(tokens, head_count, HEAD), value_a.reshape(tokens, head_count, HEAD)]
    )
    weighted = jnp.zeros((tokens, head_count, HEAD), jnp.float32)
    keep_total = jnp.zeros((head_count, tokens), jnp.float32)
    weighted, keep_total = stick_piece(
        queries, score_offset, weighted, keep_total, key_value, True, True
    )
    position = lax.axis_index("sp")
    seq_devices = lax.axis_size("sp")
    gathered = lax.all_gather(key_value, "sp", axis=1, tiled=True)

    def gathered_turn(turn_index, carried_state):
        weighted_now, keep_now = carried_state
        source = jnp.maximum(position - turn_index, 0) * tokens
        piece_pair = lax.dynamic_slice_in_dim(gathered, source, tokens, 1)
        return stick_piece(
            queries, score_offset, weighted_now, keep_now, piece_pair, False, position >= turn_index
        )

    weighted, keep_total = lax.fori_loop(1, seq_devices, gathered_turn, (weighted, keep_total))
    row_log_total = jnp.log(jnp.maximum(-jnp.expm1(keep_total), log_floor))[None]
    mixed_a = (
        head_norm(weighted, attention_norm_gain.reshape(head_count, HEAD))
        .reshape(tokens, head_count * HEAD)
        .astype(jnp.bfloat16)
    )
    forget_logits = forget_b.astype(jnp.float32) + forget_offset
    forget_log_value = (
        jnp.logaddexp(
            jnp.log(forget_floor), jnp.log1p(-forget_floor) + jax.nn.log_sigmoid(forget_logits)
        )
        + extra_log_decay[0]
    )
    key_in = (1.0 - forget_floor) * jax.nn.sigmoid(-forget_logits)
    query_rows_input = jax.nn.silu(query_b.astype(jnp.float32)).reshape(tokens, head_count, HEAD)
    value_in = input_b.astype(jnp.float32)
    fading_channel_groups = forget_log_value.reshape(tokens, head_count, HEAD)
    shaped = tuple(
        (
            array_in.reshape(tokens // BLOCK, BLOCK, head_count, HEAD)
            for array_in in (query_rows_input, forget_log_value, key_in, value_in)
        )
    )
    empty_state = jnp.zeros((head_count, HEAD, HEAD), jnp.float32)
    nearby_hidden_vector, local_out = lax.scan(recurrence_block, empty_state, shaped)
    local_out = local_out.reshape(tokens, head_count, HEAD)
    through = jnp.exp(jnp.sum(fading_channel_groups, axis=0))

    def chain_states(earlier, later):
        return (earlier[0] * later[0], later[0][:, :, None] * earlier[1] + later[1])

    identity = (jnp.ones_like(through), jnp.zeros_like(nearby_hidden_vector))
    unused_decay, incoming_state = entering(
        (through, nearby_hidden_vector), "sp", chain_states, identity
    )
    running_sum = jnp.cumsum(fading_channel_groups, axis=0)
    recurrent = local_out + jnp.einsum(
        "fby,bym->fbm",
        query_rows_input * jnp.exp(running_sum),
        incoming_state,
        precision=lax.Precision.HIGHEST,
    )
    gated_out = head_norm(recurrent, recurrence_norm_gain.reshape(head_count, HEAD)) * jax.nn.silu(
        gate_b.astype(jnp.float32).reshape(tokens, head_count, HEAD)
    )
    mixed_b = gated_out.reshape(tokens, head_count * HEAD).astype(jnp.bfloat16)
    summed = lax.psum_scatter(
        (contract_rows(mixed_a, out_a) + contract_rows(mixed_b, out_b)).astype(jnp.bfloat16),
        "tp",
        scatter_dimension=0,
        tiled=True,
    )
    layer_out = summed[None]
    return (layer_out, row_log_total)


LEAF = 16
CHUNK = 128
TILE = 256
MESH = pl.DeviceIdType.MESH


def remote(src, dst, send, recv, **where):
    return pltpu.make_async_remote_copy(
        src_ref=src, dst_ref=dst, send_sem=send, recv_sem=recv, device_id=where, device_id_type=MESH
    )


def greet(peers):
    barrier = pltpu.get_barrier_semaphore()
    for where in peers:
        pl.semaphore_signal(barrier, inc=1, device_id=where, device_id_type=MESH)
    pl.semaphore_wait(barrier, len(peers))


def nt_dot(a, b):
    return lax.dot_general(a, b, (((1,), (1,)), ((), ())), preferred_element_type=jnp.float32)


def tn_dot(a, b):
    return lax.dot_general(a, b, (((0,), (0,)), ((), ())), preferred_element_type=jnp.float32)


def grid_of(shape):
    return lax.broadcasted_iota(jnp.int32, shape, 0), lax.broadcasted_iota(jnp.int32, shape, 1)


def attend_tile(i, p_ref, shift, gain):
    here = slice(i * TILE, (i + 1) * TILE)
    r, c = grid_of((TILE, TILE))
    later = (r > c).astype(jnp.bfloat16)
    query = p_ref[here, 0:HEAD]
    total = jnp.zeros((TILE, HEAD), jnp.float32)
    keep = jnp.zeros((TILE, 1), jnp.float32)
    for j in range(i, -1, -1):
        there = slice(j * TILE, (j + 1) * TILE)
        score = nt_dot(query, p_ref[there, HEAD : 2 * HEAD]) * HEAD ** (-0.5) + shift
        soft = -(jnp.maximum(score, 0.0) + jnp.log1p(jnp.exp(-jnp.abs(score))))
        held = jnp.where(r > c, soft, 0.0) if i == j else soft
        high = held.astype(jnp.bfloat16)
        low = (held - high.astype(jnp.float32)).astype(jnp.bfloat16)
        suffix = jnp.dot(high, later, preferred_element_type=jnp.float32) + jnp.dot(
            low, later, preferred_element_type=jnp.float32
        )
        weight = jnp.exp(score + soft + suffix + keep)
        if i == j:
            weight = jnp.where(r > c, weight, 0.0)
        total += jnp.dot(
            weight.astype(jnp.bfloat16),
            p_ref[there, 2 * HEAD : 3 * HEAD],
            preferred_element_type=jnp.float32,
        )
        keep += jnp.sum(held, axis=1, keepdims=True)
    return head_norm(total, gain).astype(jnp.bfloat16), keep


def recur_chunk(p_ref, e_ref, here, state, floor, offset, gain):
    r, c = grid_of((CHUNK, CHUNK))
    lower = (r >= c).astype(jnp.float32)
    part = lambda k: p_ref[here, k * HEAD : (k + 1) * HEAD].astype(jnp.float32)
    raw = part(3)
    query = raw * jax.nn.sigmoid(raw)
    key = (1.0 - floor) * jax.nn.sigmoid(-(part(4) + offset))
    value = p_ref[here, 5 * HEAD : 6 * HEAD]
    gate = part(6)
    decay = jnp.log1p(-key) + e_ref[...].astype(jnp.float32)
    run = jnp.dot(lower, decay, precision=lax.Precision.HIGHEST, preferred_element_type=jnp.float32)
    stripes = [jnp.zeros((LEAF, CHUNK), jnp.float32)]
    for s in range(LEAF, CHUNK, LEAF):
        edge = run[s - 1 : s, :]
        near = (query[s : s + LEAF] * jnp.exp(run[s : s + LEAF] - edge)).astype(jnp.bfloat16)
        far = (key * jnp.exp(jnp.where(r < s, edge - run, -jnp.inf))).astype(jnp.bfloat16)
        stripes.append(nt_dot(near, far))
    pairs = jnp.concatenate(stripes, axis=0)
    for d in range(LEAF):
        back_key = pltpu.roll(key, d, 0) if d else key
        back_run = pltpu.roll(run, d, 0) if d else run
        gap = jnp.where(r % LEAF >= d, run - back_run, -jnp.inf)
        column = jnp.sum(query * back_key * jnp.exp(gap), axis=1, keepdims=True)
        pairs = jnp.where((r - c == d) & (r % LEAF >= d), column, pairs)
    last = run[CHUNK - 1 : CHUNK, :]
    out = jnp.dot(pairs.astype(jnp.bfloat16), value, preferred_element_type=jnp.float32)
    out += nt_dot((query * jnp.exp(run)).astype(jnp.bfloat16), state.astype(jnp.bfloat16))
    mixed = head_norm(out, gain) * (gate * jax.nn.sigmoid(gate))
    state = jnp.exp(last) * state + tn_dot(value, (key * jnp.exp(last - run)).astype(jnp.bfloat16))
    return mixed.astype(jnp.bfloat16), state


PARTS = 4


def layer_kernel(n, *refs):
    raw_ref, g_ref, xe_ref, v_ref = refs[:4]
    w_refs, o_refs = refs[4:11], refs[11:13]
    out_ref, T = refs[13:15]
    (
        X, W, O, E, x_ref, e_ref, wp, proj, ma, mb, ts, M, away, landed,
        x_send, x_recv, xx_send, xx_recv,
        o_send, o_recv, oy_send, oy_recv, oc_send, oc_recv, od_send, od_recv,
        w_send, w_recv, wy_send, wy_recv, wc_send, wc_recv, wd_send, wd_recv,
        e_send, e_recv, m_send, m_recv, b_send, b_recv, t_send, t_recv, y_send, y_recv,
        pack_sem, local_sem,
    ) = refs[15:]
    z, f, x = lax.axis_index("sp"), lax.axis_index("fs"), lax.axis_index("tp")
    core, row, side = f + 1 - 2 * (f % 2), (f + 2) % 4, 1 - x
    tokens = x_ref.shape[0]
    half = tokens // 2
    step = half // PARTS
    both = (0, 1)

    def cols(h):
        return pl.ds(pl.multiple_of(h * HEAD, HEAD), HEAD)

    packs = []
    for i, w in enumerate(w_refs):
        for h in range(n):
            packs.append(
                pltpu.make_async_copy(
                    w.at[:, h * HEAD : (h + 1) * HEAD],
                    wp.at[h, :, i * HEAD : (i + 1) * HEAD],
                    pack_sem.at[i, h],
                )
            )
    wide = o_refs[0].shape[1]
    for i, o in enumerate(o_refs):
        packs.append(
            pltpu.make_async_copy(o, O.at[z, f, :, i * wide : (i + 1) * wide], local_sem.at[i])
        )
    for copy in packs:
        copy.start()
    barrier = pltpu.get_barrier_semaphore()
    peers = [{"sp": (z + o) % n} for o in range(1, n)] + [{"fs": core}, {"fs": row}, {"tp": side}]
    for where in peers:
        pl.semaphore_signal(barrier, inc=1, device_id=where, device_id_type=MESH)

    def normalise(i, carry):
        rows = pl.ds(pl.multiple_of(i * step, step), step)
        x_ref[rows, :] = head_norm(raw_ref[rows, :].astype(jnp.float32), g_ref[...]).astype(jnp.bfloat16)
        return carry

    lax.fori_loop(0, tokens // step, normalise, 0)
    for copy in packs:
        copy.wait()
    pl.semaphore_wait(barrier, len(peers))
    own_w = pltpu.make_async_copy(wp.at[z], W.at[z, f], local_sem.at[4])
    own_w.start()

    def reach(direction, k):
        if direction == 0:
            return (z - k >= 0) & (z + 1 < n), z - 1 - k >= 0, z - k, z - 1 - k, z + 1
        return (z + k < n) & (z - 1 >= 0), z + 1 + k < n, z + k, z + 1 + k, z - 1

    def span(c):
        return pl.ds(pl.multiple_of(x * half + c * step, step), step)

    def x_copy(direction, k, c, first=False):
        _, _, out, _, to = reach(direction, k)
        src = x_ref.at[span(c)] if first else X.at[out, span(c)]
        return remote(
            src, X.at[out, span(c)], x_send.at[direction, k, c], x_recv.at[direction, k, c], sp=to
        )

    def x_wait(direction, k, c):
        block = X.at[reach(direction, k)[3], span(c)]
        return remote(block, block, x_send.at[direction, k, c], x_recv.at[direction, k, c], sp=(z + 1) % n)

    def xx_copy(direction, k, c):
        block = X.at[reach(direction, k)[3], span(c)]
        return remote(block, block, xx_send.at[direction, k, c], xx_recv.at[direction, k, c], tp=side)

    def xx_wait(direction, k, c):
        there = pl.ds(pl.multiple_of(side * half + c * step, step), step)
        block = X.at[reach(direction, k)[3], there]
        return remote(block, block, xx_send.at[direction, k, c], xx_recv.at[direction, k, c], tp=side)

    def o_copy(direction, k):
        _, _, out, _, to = reach(direction, k)
        return remote(O.at[out, f], O.at[out, f], o_send.at[direction, k], o_recv.at[direction, k], sp=to)

    def o_side(kind, direction, k, own=False):
        block = z if own else reach(direction, k)[3]
        send, recv = ((oy_send, oy_recv), (oc_send, oc_recv), (od_send, od_recv))[kind]
        piece = O.at[block, row if kind == 2 else f]
        where = {"fs": row if kind == 0 else core}
        return remote(piece, piece, send.at[direction, k], recv.at[direction, k], **where)

    def o_own(kind):
        return o_side(kind, 2, 0, own=True)

    def w_copy(o):
        return remote(wp.at[(z + o) % n], W.at[z, f], w_send.at[o], w_recv.at[o], sp=(z + o) % n)

    def e_copy(o):
        return remote(e_ref.at[:, cols((z + o) % n)], E.at[z], e_send.at[o], e_recv.at[o], sp=(z + o) % n)

    def w_side(kind, o):
        block = (z - o + n) % n
        src = wp.at[z] if o == 0 else W.at[block, f]
        if kind == 0:
            return remote(src, W.at[block, f], wy_send.at[o], wy_recv.at[o], fs=row)
        if kind == 1:
            return remote(src, W.at[block, f], wc_send.at[o], wc_recv.at[o], fs=core)
        return remote(W.at[block, row], W.at[block, row], wd_send.at[o], wd_recv.at[o], fs=core)

    for d in both:
        @pl.when(reach(d, 0)[0])
        def _(d=d):
            for c in range(PARTS):
                x_copy(d, 0, c, True).start()
    for o in range(1, n):
        w_copy(o).start()
    for kind in both:
        w_side(kind, 0).start()
    local = [
        pltpu.make_async_copy(x_ref, X.at[z], local_sem.at[2]),
        pltpu.make_async_copy(e_ref.at[:, cols(z)], E.at[z], local_sem.at[3]),
    ]
    local[0].start()
    e_ref[...] = xe_ref[...].astype(jnp.bfloat16)

    def o_begin(direction, when):
        @pl.when(when & reach(direction, 0)[0])
        def _():
            o_copy(direction, 0).start()

    local[0].wait()
    own_w.wait()

    def project(block):
        rows = X[block]
        weights = W[...].reshape(rows.shape[1], W.shape[3])
        made = jnp.dot(rows, weights, preferred_element_type=jnp.float32)
        at = pl.ds(pl.multiple_of(block * tokens, tokens), tokens)
        proj[at, :] = made.astype(jnp.bfloat16)

    def gather_step(k, carry):
        for d in both:
            @pl.when((k < n - 1) & reach(d, k)[1])
            def _(d=d):
                for c in range(PARTS):
                    x_wait(d, k, c).wait_recv()

                    @pl.when(reach(d, k + 1)[0])
                    def _(c=c):
                        x_copy(d, k + 1, c).start()
                    xx_copy(d, k, c).start()

        @pl.when(k == n - 2)
        def _():
            local[1].start()
            for o in range(1, n):
                e_copy(o).start()

        o_begin(0, k == n - 2)
        o_begin(1, k == n - 2)

        @pl.when(k == 0)
        def _():
            for o in range(1, n):
                w_copy(o).wait_recv()
                for kind in both:
                    w_side(kind, o).start()
            for kind in both:
                o_own(kind).start()
            for o in range(n):
                w_side(0, o).wait_recv()
                w_side(2, o).start()
            for o in range(n):
                w_side(1, o).wait_recv()
                w_side(2, o).wait_recv()

        @pl.when(z - k >= 0)
        def _():
            @pl.when(k > 0)
            def _():
                for c in range(PARTS):
                    xx_wait(0, k - 1, c).wait_recv()
            project(z - k)

        @pl.when((k > 0) & (z + k < n))
        def _():
            for c in range(PARTS):
                xx_wait(1, k - 1, c).wait_recv()
            project(z + k)
        return carry

    lax.fori_loop(0, n, gather_step, 0)

    def o_tick(k):
        for d in both:
            @pl.when(reach(d, k)[1])
            def _(d=d):
                o_copy_in = O.at[reach(d, k)[3], f]
                remote(o_copy_in, o_copy_in, o_send.at[d, k], o_recv.at[d, k], sp=(z + 1) % n).wait_recv()
                if k + 1 < n - 1:
                    @pl.when(reach(d, k + 1)[0])
                    def _():
                        o_copy(d, k + 1).start()
                for kind in both:
                    o_side(kind, d, k).start()

    def m_copy(o):
        return remote(ma.at[(z + o) % n], M.at[0, z], m_send.at[o], m_recv.at[o], sp=(z + o) % n)

    def b_copy(o):
        return remote(mb.at[(z + o) % n], M.at[1, z], b_send.at[o], b_recv.at[o], sp=(z + o) % n)

    def t_copy(o):
        return remote(ts.at[(z + o) % n], T.at[z], t_send.at[o], t_recv.at[o], sp=(z + o) % n)

    param = lambda i: v_ref[i, pl.ds(z, 1), :]
    shift = param(0)[:, 0:1]
    for i in range(n):
        mixed, keep = attend_tile(i, proj, shift, param(1))
        ma[i] = mixed
        total = jnp.log(jnp.maximum(1.0 - jnp.exp(keep), log_floor))
        ts[i] = jnp.broadcast_to(total, (tokens, HEAD)).T[0:8, :]
    o_tick(0)
    local[1].wait()
    for o in range(1, n):
        e_copy(o).wait_recv()
    floor, offset, gain = param(3), param(4), param(2)
    per = tokens // CHUNK

    def chunk(i, state):
        here = pl.ds(pl.multiple_of(i * CHUNK, CHUNK), CHUNK)
        at = pl.ds(pl.multiple_of((i % per) * CHUNK, CHUNK), CHUNK)
        extra = E.at[i // per, at]
        mixed, state = recur_chunk(proj, extra, here, state, floor, offset, gain)
        mb[i // per, at, :] = mixed
        return state

    state = jnp.zeros((HEAD, HEAD), jnp.float32)
    count = per * n
    state = lax.fori_loop(0, count // 2, chunk, state)
    for o in range(1, n):
        m_copy(o).start()
    for o in range(1, n):
        t_copy(o).start()
    if n > 2:
        o_tick(1)
    lax.fori_loop(count // 2, count, chunk, state)
    mine = [
        pltpu.make_async_copy(ma.at[z], M.at[0, z], local_sem.at[5]),
        pltpu.make_async_copy(mb.at[z], M.at[1, z], local_sem.at[6]),
        pltpu.make_async_copy(ts.at[z], T.at[z], local_sem.at[7]),
    ]
    for copy in mine:
        copy.start()
    for o in range(1, n):
        b_copy(o).start()
    o_own(0).wait_recv()
    o_own(2).start()
    for k in range(2, n - 1):
        o_tick(k)
    o_own(1).wait_recv()
    o_own(2).wait_recv()
    for copy in mine:
        copy.wait()
    for o in range(1, n):
        m_copy(o).wait()
        b_copy(o).wait()

    shorter = jnp.minimum(z, n - 1 - z)

    def hop_of(s):
        t = s - 1
        paired = t < 2 * shorter
        k = jnp.where(paired, t // 2, t - shorter)
        d = jnp.where(paired, t % 2, jnp.where(z > n - 1 - z, 0, 1))
        return d, k, jnp.where(d == 0, z - 1 - k, z + 1 + k)

    def o_late(kind, s):
        d, k, block = hop_of(s)
        send, recv = ((oy_send, oy_recv), (oc_send, oc_recv), (od_send, od_recv))[kind]
        piece = O.at[block, row if kind == 2 else f]
        where = {"fs": row if kind == 0 else core}
        return remote(piece, piece, send.at[d, k], recv.at[d, k], **where)

    def rows_of(which):
        rows = pl.ds(pl.multiple_of(which * half, half), half)
        return jnp.concatenate([M[g, k, rows, :] for g in both for k in range(n)], axis=1)

    width = out_ref.shape[1] // n

    def y_copy(j):
        return remote(away.at[j], landed.at[j], y_send.at[j], y_recv.at[j], tp=side)

    def weights_of(block):
        return O[block].reshape(width, 2 * wide)

    theirs = rows_of(side)
    o_late(0, 1).wait_recv()
    o_late(2, 1).start()
    for j in range(n):
        if j:
            o_late(1, j).wait_recv()
            o_late(2, j).wait_recv()
        away[j] = nt_dot(theirs, weights_of(hop_of(j)[2] if j else z)).astype(jnp.bfloat16)
        if j:
            y_copy(j - 1).start()
            if j + 1 < n:
                o_late(0, j + 1).wait_recv()
                o_late(2, j + 1).start()
    ours = rows_of(x)
    for j in range(n):
        block = hop_of(j)[2] if j else z
        piece = nt_dot(ours, weights_of(block))
        if j == 0:
            y_copy(n - 1).start()
        y_copy(j).wait_recv()
        piece += landed[j].astype(jnp.float32)
        out_ref[:, pl.ds(pl.multiple_of(block * width, width), width)] = piece.astype(jnp.bfloat16)
    for j in range(n):
        y_copy(j).wait_send()
    for o in range(n):
        for kind in range(3):
            w_side(kind, o).wait_send()
    for o in range(1, n):
        t_copy(o).wait()
        e_copy(o).wait_send()
        w_copy(o).wait_send()
    for kind in range(3):
        o_own(kind).wait_send()
    for k in range(n - 1):
        for d in both:
            @pl.when(reach(d, k)[1])
            def _(d=d, k=k):
                for c in range(PARTS):
                    xx_copy(d, k, c).wait_send()
                for kind in range(3):
                    o_side(kind, d, k).wait_send()

            @pl.when(reach(d, k)[0])
            def _(d=d, k=k):
                for c in range(PARTS):
                    x_copy(d, k, c).wait_send()
                o_copy(d, k).wait_send()


VMEM = pl.BlockSpec(memory_space=pltpu.VMEM)
ANY = pl.BlockSpec(memory_space=pl.ANY)
DMA = pltpu.SemaphoreType.DMA


def on_device_heads(
    n,
    input_layer_rows,
    input_norm_gain,
    query_weight_attention,
    key_weight_attention,
    value_weight_attention,
    query_weight_recurrent,
    forget_weight_recurrent,
    value_weight_recurrent,
    gate_weight_recurrent,
    output_weight_attention,
    emitted_projection_linear_scan,
    score_offset,
    attention_norm_gain,
    recurrence_norm_gain,
    forget_floor,
    forget_offset,
    extra_log_decay,
):
    _, tokens, depth = input_layer_rows.shape
    groups = lax.axis_size("fs")
    share, columns = query_weight_attention.shape
    width = 7 * HEAD
    half = tokens // 2
    vectors = jnp.stack(
        [jnp.broadcast_to(score_offset[:, None], (n, HEAD))]
        + [
            v.reshape(n, HEAD)
            for v in (attention_norm_gain, recurrence_norm_gain, forget_floor, forget_offset)
        ]
    )
    bf = lambda *shape: pltpu.VMEM(shape, jnp.bfloat16)
    layer_out, T = pl.pallas_call(
        functools.partial(layer_kernel, n),
        out_shape=(
            jax.ShapeDtypeStruct((half, depth), jnp.bfloat16),
            jax.ShapeDtypeStruct((n, 8, tokens), jnp.float32),
        ),
        in_specs=[VMEM] * 4 + [ANY] * 9,
        out_specs=(VMEM,) * 2,
        scratch_shapes=[
            bf(n, tokens, depth),
            bf(n, groups, share, width),
            bf(n, groups, share, 2 * columns),
            bf(n, tokens, HEAD),
            bf(tokens, depth),
            bf(tokens, columns),
            bf(n, share, width),
            bf(n * tokens, width),
            bf(n, tokens, HEAD),
            bf(n, tokens, HEAD),
            pltpu.VMEM((n, 8, tokens), jnp.float32),
            bf(2, n, tokens, HEAD),
            bf(n, half, depth // n),
            bf(n, half, depth // n),
        ]
        + [DMA((2, n, PARTS))] * 4
        + [DMA((2, n))] * 2
        + [DMA((3, n))] * 6
        + [DMA((n,))] * 18
        + [DMA((7, n)), DMA((8,))],
        compiler_params=pltpu.CompilerParams(
            collective_id=0, has_side_effects=True, vmem_limit_bytes=56 * 1024 * 1024
        ),
    )(
        input_layer_rows[0],
        input_norm_gain[None],
        extra_log_decay[0],
        vectors,
        query_weight_attention,
        key_weight_attention,
        value_weight_attention,
        query_weight_recurrent,
        forget_weight_recurrent,
        value_weight_recurrent,
        gate_weight_recurrent,
        output_weight_attention,
        emitted_projection_linear_scan,
    )
    return (layer_out[None], T[:, 0, :][None])


def solution(mesh):
    n = mesh.shape["sp"]
    heads_fit = mesh.shape["fs"] == 4 and mesh.shape["tp"] == 2 and n > 1

    def on_device(*args):
        if heads_fit and args[11].shape[0] == n and args[0].shape[1] == TILE:
            return on_device_heads(n, *args)
        return on_device_general(*args)

    return jax.shard_map(
        on_device,
        mesh=mesh,
        in_specs=(
            P("fs", "sp", None),
            P(),
            P(("sp", "fs"), "tp"),
            P(("sp", "fs"), "tp"),
            P(("sp", "fs"), "tp"),
            P(("sp", "fs"), "tp"),
            P(("sp", "fs"), "tp"),
            P(("sp", "fs"), "tp"),
            P(("sp", "fs"), "tp"),
            P(("sp", "fs"), "tp"),
            P(("sp", "fs"), "tp"),
            P("tp"),
            P("tp"),
            P("tp"),
            P("tp"),
            P("tp"),
            P("fs", "sp", "tp"),
        ),
        out_specs=(P("fs", ("sp", "tp"), None), P("fs", "tp", "sp")),
        check_vma=False,
    )
```
